32 devices in a mesh: ra: 4 (over y, x), cb: 8 (over z, core).
Axes of the slice: x: 2, y: 2, z: 4, core: 2. Of those that a mesh axis runs over, the one named last changes fastest.
Arguments:
- tokens: bfloat16 [256, 4096], P(None, 'ra'), may hold values from -20 to 20, as said below
- norm_gain: float32 [2, 4096], P(None, 'ra'), may hold values from 0.1 to 1.9
- gate_weight: bfloat16 [2, 4096, 11008], P(None, 'ra', 'cb'), may hold values from -0.09375 to 0.09375
- value_weight: bfloat16 [2, 4096, 11008], P(None, 'ra', 'cb'), may hold values from -0.09375 to 0.09375
- gate_taps: float32 [2, 3, 11008], P(None, None, 'cb'), may hold values from -3.5 to 3.5
- value_taps: float32 [2, 3, 11008], P(None, None, 'cb'), may hold values from -3.5 to 3.5
- down_weight: bfloat16 [2, 11008, 4096], P(None, 'cb', 'ra'), may hold values from -0.0546875 to 0.0546875
Outputs:
- mixed: bfloat16 [256, 4096], P(None, 'ra')
The draws below stay inside these ranges and needn't reach their ends.
Inputs may be any that keep to these rules, and one draw needn't show every extreme that they name: tokens have features drawn around zero with a scale that varies by blocks of features between about 0.3 and 3.3.
All inputs are finite; a program needn't handle non-finite values.
Results may differ from the reference program's by a relative error of at most 0.0075.
Values may be sent and summed in bfloat16 or wider, within the bound.
No kernel may reach another device: no remote copies, remote signals or barrier semaphores. Data moves between devices by JAX's collectives and lax.ppermute only.
A program may use at most 128 MiB of HBM per device.

```python
import jax
import jax.numpy as jnp
from jax import lax

D = 4096
FF = 11008
KERNEL = 3
LAYERS = 2
TOKENS = 256


def draw_tokens(key, part):
    base_key, scale_key = jax.random.split(jax.random.fold_in(key, 11))
    block_scales = jnp.exp(jax.random.uniform(scale_key, (64,), jnp.float32, -1.2, 1.2))
    column_scales = jnp.repeat(block_scales, D // 64)
    base = jnp.clip(jax.random.normal(base_key, (TOKENS, D), jnp.float32), -6.0, 6.0)
    return (base * column_scales[None, :]).astype(jnp.bfloat16)


def block_levels(stream_key, shape, pieces, least, top_value):
    factor_of = 1.0
    for position, blocks in pieces:
        draws = jax.random.uniform(jax.random.fold_in(jax.random.fold_in(stream_key, 6), position), (blocks,), jnp.float32, least / len(pieces), top_value / len(pieces))
        factor_of = factor_of * jnp.repeat(jnp.exp(draws), shape[position] // blocks).reshape((-1,) + (1,) * (len(shape) - 1 - position))
    return factor_of


def bell_draw(stream_key, dims, spread, most, shards=(), held_as=jnp.bfloat16):
    drawn = spread * jax.random.normal(stream_key, dims, jnp.float32)
    if shards:
        drawn = drawn * block_levels(stream_key, dims, shards, -0.22, 0.18)
    return jnp.clip(drawn, -most, most).astype(held_as)


def setup_inputs(seed: int = 0) -> dict:
    keys = jax.random.split(jax.random.key(seed), 8)
    return {
        "tokens": draw_tokens(jax.random.fold_in(keys[7], 71), 0),
        "norm_gain": jnp.clip(1.0 + 0.18 * jax.random.normal(keys[1], (LAYERS, D), jnp.float32), 0.1, 1.9),
        "gate_weight": bell_draw(keys[2], (LAYERS, D, FF), D ** -0.5, 0.09375, ((1, 4), (2, 8))),
        "value_weight": bell_draw(keys[3], (LAYERS, D, FF), D ** -0.5, 0.09375, ((1, 4), (2, 8))),
        "gate_taps": bell_draw(keys[4], (LAYERS, KERNEL, FF), KERNEL ** -0.5, 3.5, ((2, 8),), jnp.float32),
        "value_taps": bell_draw(keys[5], (LAYERS, KERNEL, FF), KERNEL ** -0.5, 3.5, ((2, 8),), jnp.float32),
        "down_weight": bell_draw(keys[6], (LAYERS, FF, D), FF ** -0.5, 0.0546875, ((1, 8), (2, 4))),
    }


epsilon = 1e-06

def causal_conv(signal, kernel_taps):
    length = signal.shape[0]
    width = kernel_taps.shape[0]
    padded = jnp.concatenate([jnp.zeros((width - 1, signal.shape[1]), jnp.float32), signal], axis=0)
    result = jnp.zeros(signal.shape, jnp.float32)
    for offset in range(width):
        result = result + kernel_taps[offset] * padded[offset:offset + length]
    return result

def reference(tokens, norm_gain, gate_weight, value_weight, gate_taps, value_taps, down_weight):
    stream = tokens
    for layer_index in range(LAYERS):
        current = stream.astype(jnp.float32)
        inverse_rms = lax.rsqrt(lax.optimization_barrier(jnp.sum(current * current, axis=1, keepdims=True)) / D + epsilon)
        scaled = (current * norm_gain[layer_index]).astype(jnp.bfloat16)
        gate_lin = jnp.dot(scaled, gate_weight[layer_index], preferred_element_type=jnp.float32) * inverse_rms
        value_lin = jnp.dot(scaled, value_weight[layer_index], preferred_element_type=jnp.float32) * inverse_rms
        gate_conv = causal_conv(gate_lin, gate_taps[layer_index])
        value_conv = causal_conv(value_lin, value_taps[layer_index])
        hidden = (jax.nn.silu(gate_conv) * value_conv).astype(jnp.bfloat16)
        branch = jnp.dot(hidden, down_weight[layer_index], preferred_element_type=jnp.float32)
        stream = (0.5 * current + branch).astype(jnp.bfloat16)
    return stream
```

```python
import jax
import jax.numpy as jnp
from jax import lax
from jax.sharding import PartitionSpec as P

epsilon = 1e-06
F32 = jnp.float32
BF16 = jnp.bfloat16


def conv_lanes(signal, taps):
    width = taps.shape[0]
    length = signal.shape[1]
    padded = jnp.pad(signal, ((0, 0), (width - 1, 0)))
    result = jnp.zeros(signal.shape, F32)
    for offset in range(width):
        result = result + taps[offset][:, None] * padded[:, offset : offset + length]
    return result


def make_body(mesh):
    n_a = mesh.shape["ra"]
    n_c = mesh.shape["cb"]
    n_z = n_c // 2

    def peer(i, s, n):
        return i ^ s if n & (n - 1) == 0 else (i + s) % n

    def source(i, s, n):
        return i ^ s if n & (n - 1) == 0 else (i - s) % n

    def send_a(value, s):
        return lax.ppermute(value, "ra", [(i, peer(i, s, n_a)) for i in range(n_a)])

    def send_z(value, s):
        pairs = [(z * 2 + k, peer(z, s, n_z) * 2 + k) for z in range(n_z) for k in range(2)]
        return lax.ppermute(value, "cb", pairs)

    def send_core(value):
        return lax.ppermute(value, "cb", [(i, i ^ 1) for i in range(n_c)])

    def body(tokens, norm_gain, gate_weight, value_weight, gate_taps, value_taps, down_weight):
        layers, width, units = gate_weight.shape
        positions = tokens.shape[0]
        total_width = width * n_a
        piece = -(-(-(-units // n_a)) // 8) * 8
        a = lax.axis_index("ra")
        c = lax.axis_index("cb")
        z, core = c // 2, c % 2
        half = positions // 2
        span = half // n_z

        def start(p):
            return jnp.minimum(p * piece, units - piece)

        stream = tokens
        for layer in range(layers):
            current = stream.astype(F32)
            squares = jnp.sum(current * current, axis=1)[None, :]
            scaled = (current * norm_gain[layer]).astype(BF16)
            total = squares
            for s in range(1, n_a):
                total = total + send_a(squares, s)
            contract = (((0,), (1,)), ((), ()))
            gate = lax.dot_general(gate_weight[layer], scaled, contract, preferred_element_type=F32)
            value = lax.dot_general(value_weight[layer], scaled, contract, preferred_element_type=F32)

            def cut(p):
                return jnp.stack(
                    [
                        lax.dynamic_slice_in_dim(gate, start(p), piece, 0),
                        lax.dynamic_slice_in_dim(value, start(p), piece, 0),
                    ]
                )

            both = cut(a)
            for s in range(1, n_a):
                both = both + send_a(cut(peer(a, s, n_a)).astype(BF16), s).astype(F32)
            both = both * lax.rsqrt(total / total_width + epsilon)
            my = start(a)
            g_taps = lax.dynamic_slice_in_dim(gate_taps[layer], my, piece, 1)
            v_taps = lax.dynamic_slice_in_dim(value_taps[layer], my, piece, 1)
            gate_conv = conv_lanes(both[0], g_taps)
            value_conv = conv_lanes(both[1], v_taps)
            mine = (jax.nn.silu(gate_conv) * value_conv).astype(BF16)
            hidden = jnp.zeros((units, positions), BF16)
            hidden = lax.dynamic_update_slice_in_dim(hidden, mine, my, 0)
            for s in range(1, n_a):
                other = send_a(mine, s)
                hidden = lax.dynamic_update_slice_in_dim(
                    hidden, other, start(source(a, s, n_a)), 0
                )
            partial = lax.dot_general(
                hidden,
                down_weight[layer],
                (((0,), (0,)), ((), ())),
                preferred_element_type=F32,
            )
            away = lax.dynamic_slice_in_dim(partial, (1 - core) * half, half, 0).astype(BF16)
            kept = lax.dynamic_slice_in_dim(partial, core * half, half, 0)
            kept = kept + send_core(away).astype(F32)
            branch = lax.dynamic_slice_in_dim(kept, z * span, span, 0)
            for s in range(1, n_z):
                out = lax.dynamic_slice_in_dim(kept, peer(z, s, n_z) * span, span, 0)
                branch = branch + send_z(out.astype(BF16), s).astype(F32)
            old = lax.dynamic_slice_in_dim(stream, core * half + z * span, span, 0)
            fresh = (0.5 * old.astype(F32) + branch).astype(BF16)
            mid = jnp.zeros((half, width), BF16)
            mid = lax.dynamic_update_slice_in_dim(mid, fresh, z * span, 0)
            for s in range(1, n_z):
                mid = lax.dynamic_update_slice_in_dim(
                    mid, send_z(fresh, s), source(z, s, n_z) * span, 0
                )
            far = send_core(mid)
            stream = jnp.where(
                core == 0,
                jnp.concatenate([mid, far], axis=0),
                jnp.concatenate([far, mid], axis=0),
            )
        return stream

    return body


def solution(mesh):
    return jax.shard_map(
        make_body(mesh),
        mesh=mesh,
        in_specs=(
            P(None, "ra"),
            P(None, "ra"),
            P(None, "ra", "cb"),
            P(None, "ra", "cb"),
            P(None, None, "cb"),
            P(None, None, "cb"),
            P(None, "cb", "ra"),
        ),
        out_specs=P(None, "ra"),
        check_vma=False,
    )
```

```python
import functools

import jax
import jax.numpy as jnp
from jax import lax
from jax.experimental import pallas as pl
from jax.experimental.pallas import tpu as pltpu
from jax.sharding import PartitionSpec as P

epsilon = 1e-06
F32 = jnp.float32
BF16 = jnp.bfloat16
EXTRA = 8
CHUNKS = 1
VMEM = pl.BlockSpec(memory_space=pltpu.VMEM)


def cost(flops, moved):
    return pl.CostEstimate(flops=int(flops), bytes_accessed=int(moved), transcendentals=0)


def up_kernel(near_ref, far_ref, side_ref, gain_ref, gate_ref, value_ref, out_ref, rows_ref, scaled_ref, *, starts, piece, joined):
    slot = pl.program_id(0)

    @pl.when(slot == 0)
    def _():
        if joined:
            half = near_ref.shape[0]
            side = side_ref[0]
            rows_ref[pl.ds(pl.multiple_of(side * half, half), half), :] = near_ref[...]
            rows_ref[pl.ds(pl.multiple_of((1 - side) * half, half), half), :] = far_ref[...]
            current = rows_ref[...].astype(F32)
        else:
            current = near_ref[...].astype(F32)
        scaled_ref[...] = (current * gain_ref[...]).astype(BF16)
        squares = current * current
        width = squares.shape[1]
        folded = squares[:, :128]
        for k in range(1, width // 128):
            folded = folded + squares[:, k * 128 : (k + 1) * 128]
        total = jnp.sum(folded.T, axis=0, keepdims=True)
        high = total.astype(BF16)
        low = (total - high.astype(F32)).astype(BF16)
        row = lax.broadcasted_iota(jnp.int32, (EXTRA, total.shape[1]), 0)
        tail = jnp.where(row == 0, high.astype(F32), jnp.where(row == 1, low.astype(F32), 0.0))
        rows_ref[0:EXTRA, 0 : total.shape[1]] = tail.astype(BF16)

    scaled = scaled_ref[...]
    contract = (((1,), (1,)), ((), ()))
    out_ref[0, 0:piece, :] = lax.dot_general(
        gate_ref[...], scaled, contract, preferred_element_type=F32
    ).astype(BF16)
    out_ref[0, piece : 2 * piece, :] = lax.dot_general(
        value_ref[...], scaled, contract, preferred_element_type=F32
    ).astype(BF16)
    out_ref[0, 2 * piece : 2 * piece + EXTRA, :] = rows_ref[0:EXTRA, 0 : out_ref.shape[2]]


def act_kernel(parts_ref, taps_ref, prior_ref, out_ref, held_ref, *, piece, width, first, layer, kernel):
    n = parts_ref.shape[0]
    total = parts_ref[0].astype(F32)
    for s in range(1, n):
        total = total + parts_ref[s].astype(F32)
    tail = total[2 * piece : 2 * piece + EXTRA]
    squares = tail[0:1] + tail[1:2]
    inverse = lax.rsqrt(squares / width + epsilon)
    lin = total[: 2 * piece] * inverse
    if held_ref is not None:
        held_ref[...] = lin
    lane = lax.broadcasted_iota(jnp.int32, (piece, lin.shape[1]), 1)

    def conv(kind):
        current = lin[kind * piece : (kind + 1) * piece]
        result = None
        for k in range(kernel):
            shift = kernel - 1 - k
            column = (layer * 2 + kind) * kernel + k
            tap = taps_ref[:, column : column + 1]
            moved = current
            if shift:
                moved = pltpu.roll(current, shift, 1)
                if first:
                    fill = jnp.zeros_like(moved)
                else:
                    fill = pltpu.roll(prior_ref[kind * piece : (kind + 1) * piece, :], shift, 1)
                moved = jnp.where(lane < shift, fill, moved)
            term = tap * moved
            result = term if result is None else result + term
        return result

    gate, value = conv(0), conv(1)
    hidden = (gate / (1.0 + jnp.exp(-gate)) * value).astype(BF16)
    for s in range(n):
        out_ref[s] = hidden


def down_kernel(hidden_ref, weight_ref, side_ref, away_ref, kept_ref, total_ref, *, starts, piece):
    total = None
    for s, begin in enumerate(starts):
        skip = s * piece - begin
        if skip >= piece:
            continue
        term = lax.dot_general(
            hidden_ref[s, skip:piece, :],
            weight_ref[begin + skip : begin + piece, :],
            (((0,), (0,)), ((), ())),
            preferred_element_type=F32,
        )
        total = term if total is None else total + term
    total_ref[...] = total
    half = away_ref.shape[0]
    side = side_ref[0]
    away_ref[...] = total_ref[pl.ds(pl.multiple_of((1 - side) * half, half), half), :].astype(BF16)
    kept_ref[...] = total_ref[pl.ds(pl.multiple_of(side * half, half), half), :]


def make_body(mesh):
    n_a = mesh.shape["ra"]
    n_c = mesh.shape["cb"]
    n_z = n_c // 2
    z_groups = [[z * 2 + k for z in range(n_z)] for k in range(2)]

    def trade_a(value):
        return lax.all_to_all(value, "ra", 0, 0)

    def trade_z(value):
        return lax.all_to_all(value, "cb", 0, 0, axis_index_groups=z_groups)

    def trade_core(value):
        return lax.ppermute(value, "cb", [(i, i ^ 1) for i in range(n_c)])

    def body(tokens, norm_gain, gate_weight, value_weight, gate_taps, value_taps, down_weight):
        layers, width, units = gate_weight.shape
        kernel = gate_taps.shape[1]
        count = tokens.shape[0] // CHUNKS
        piece = -(-(-(-units // n_a)) // 8) * 8
        starts = [min(p * piece, units - piece) for p in range(n_a)]
        even = starts[-1] == (n_a - 1) * piece
        a = lax.axis_index("ra")
        c = lax.axis_index("cb")
        z, core = c // 2, c % 2
        side = core.astype(jnp.int32).reshape(1)
        half = count // 2
        span = half // n_z
        gate_rows = gate_weight.transpose(0, 2, 1)
        value_rows = value_weight.transpose(0, 2, 1)
        if not even:
            index = jnp.concatenate([jnp.arange(b, b + piece) for b in starts])
            gate_rows = gate_rows[:, index]
            value_rows = value_rows[:, index]

        my = jnp.minimum(a * piece, units - piece)
        taps = jnp.stack([gate_taps, value_taps], axis=1).reshape(layers * 2 * kernel, units)
        taps = lax.dynamic_slice_in_dim(taps, my, piece, 1).T

        def up(layer, near, far):
            joined = far is not None
            rows = 2 * piece + EXTRA
            body_fn = functools.partial(up_kernel, starts=starts, piece=piece, joined=joined)
            if not joined:
                far = near
            whole = lambda shape: pl.BlockSpec(shape, lambda i: (0,) * len(shape))
            return pl.pallas_call(
                body_fn,
                grid=(n_a,),
                in_specs=[
                    whole(near.shape),
                    whole(far.shape),
                    pl.BlockSpec(memory_space=pltpu.SMEM),
                    whole((1, width)),
                    pl.BlockSpec((None, piece, width), lambda i: (layer, i, 0)),
                    pl.BlockSpec((None, piece, width), lambda i: (layer, i, 0)),
                ],
                out_specs=pl.BlockSpec((1, rows, count), lambda i: (i, 0, 0)),
                out_shape=jax.ShapeDtypeStruct((n_a, rows, count), BF16),
                scratch_shapes=[
                    pltpu.VMEM((count, max(width, count)), BF16),
                    pltpu.VMEM((count, width), BF16),
                ],
                cost_estimate=cost(4 * units * width * count, 4 * units * width),
                name=f"up{layer}",
            )(near, far, side, norm_gain[layer][None, :], gate_rows, value_rows)

        def act(layer, chunk, parts, prior):
            first, last = chunk == 0, chunk == CHUNKS - 1
            args = [parts, taps]
            if not first:
                args.append(prior)
            shapes = [jax.ShapeDtypeStruct((n_a, piece, count), BF16)]
            if not last:
                shapes.append(jax.ShapeDtypeStruct((2 * piece, count), F32))

            def body_fn(*refs):
                refs = list(refs)
                if first:
                    refs.insert(2, None)
                if last:
                    refs.append(None)
                act_kernel(
                    *refs, piece=piece, width=width * n_a, first=first, layer=layer, kernel=kernel
                )

            out = pl.pallas_call(
                body_fn,
                in_specs=[VMEM] * len(args),
                out_specs=[VMEM] * len(shapes),
                out_shape=shapes,
                cost_estimate=cost(60 * 2 * piece * count, 4 * n_a * piece * count),
                name=f"act{layer}_{chunk}",
            )(*args)
            return (out[0], None) if last else out

        def down(layer, hidden):
            return pl.pallas_call(
                functools.partial(down_kernel, starts=starts, piece=piece),
                grid=(1,),
                in_specs=[
                    pl.BlockSpec((n_a, piece, count), lambda i: (0, 0, 0)),
                    pl.BlockSpec((None, units, width), lambda i: (layer, 0, 0)),
                    pl.BlockSpec(memory_space=pltpu.SMEM),
                ],
                out_specs=[pl.BlockSpec((half, width), lambda i: (0, 0))] * 2,
                out_shape=[
                    jax.ShapeDtypeStruct((half, width), BF16),
                    jax.ShapeDtypeStruct((half, width), F32),
                ],
                scratch_shapes=[pltpu.VMEM((count, width), F32)],
                cost_estimate=cost(2 * units * width * count, 2 * units * width),
                name=f"down{layer}",
            )(hidden, down_weight, side)

        near = [tokens[i * count : (i + 1) * count] for i in range(CHUNKS)]
        far = [None] * CHUNKS
        old = [
            lax.dynamic_slice_in_dim(near[i], core * half + z * span, span, 0)
            for i in range(CHUNKS)
        ]
        for layer in range(layers):
            prior = None
            for i in range(CHUNKS):
                parts = trade_a(up(layer, near[i], far[i]))
                mine, prior = act(layer, i, parts, prior)
                away, kept = down(layer, trade_a(mine))
                total = kept + trade_core(away).astype(F32)
                terms = trade_z(total.astype(BF16).reshape(n_z, span, width))
                branch = jnp.sum(terms.astype(F32), axis=0)
                old[i] = (0.5 * old[i].astype(F32) + branch).astype(BF16)
                spread = jnp.broadcast_to(old[i][None], (n_z, span, width))
                near[i] = trade_z(spread).reshape(half, width)
                far[i] = trade_core(near[i])
        parts = []
        for i in range(CHUNKS):
            parts.append(jnp.where(core == 0, near[i], far[i]))
            parts.append(jnp.where(core == 0, far[i], near[i]))
        return jnp.concatenate(parts, axis=0)

    return body


def solution(mesh):
    return jax.shard_map(
        make_body(mesh),
        mesh=mesh,
        in_specs=(
            P(None, "ra"),
            P(None, "ra"),
            P(None, "ra", "cb"),
            P(None, "ra", "cb"),
            P(None, None, "cb"),
            P(None, None, "cb"),
            P(None, "cb", "ra"),
        ),
        out_specs=P(None, "ra"),
        check_vma=False,
    )
```

```python
import jax
import jax.numpy as jnp
from jax import lax
from jax.experimental import pallas as pl
from jax.experimental.pallas import tpu as pltpu
from jax.sharding import PartitionSpec as P


epsilon = 1e-06
F32 = jnp.float32
BF16 = jnp.bfloat16
EXTRA = 8
SPLITS = 2
MIB = 1 << 20
WIDE = 16
VMEM = pl.BlockSpec(memory_space=pltpu.VMEM)
SMEM = pl.BlockSpec(memory_space=pltpu.SMEM)
HBM = pl.BlockSpec(memory_space=pltpu.HBM)


def call(body, args, specs, shapes, flops, moved, scratch=(), room=16):
    return pl.pallas_call(
        body,
        in_specs=specs,
        out_specs=[VMEM] * len(shapes),
        out_shape=[jax.ShapeDtypeStruct(*shape) for shape in shapes],
        scratch_shapes=scratch,
        cost_estimate=pl.CostEstimate(
            flops=int(flops), bytes_accessed=int(moved), transcendentals=0
        ),
        compiler_params=pltpu.CompilerParams(vmem_limit_bytes=room * MIB),
    )(*args)


def aligned(value, step=8):
    return pl.multiple_of(value, step)


def prepare(current, gain, scaled_ref, tail_ref):
    scaled_ref[...] = (current * gain).astype(BF16)
    squares = current * current
    folded = squares[:, :128]
    for k in range(1, squares.shape[1] // 128):
        folded = folded + squares[:, k * 128 : (k + 1) * 128]
    total = jnp.sum(folded.T, axis=0, keepdims=True)
    high = total.astype(BF16).astype(F32)
    low = total - high
    row = lax.broadcasted_iota(jnp.int32, (EXTRA, total.shape[1]), 0)
    tail_ref[...] = jnp.where(row == 0, high, jnp.where(row == 1, low, 0.0)).astype(BF16)


def load_rows(pieces, side_ref, rows_ref):
    if len(pieces) == 1:
        return pieces[0][...].astype(F32)
    near, far = pieces
    half = near.shape[0]
    side = side_ref[0] & 1
    rows_ref[pl.ds(aligned(side * half, half), half), :] = near[...]
    rows_ref[pl.ds(aligned((1 - side) * half, half), half), :] = far[...]
    return rows_ref[...].astype(F32)


def make_body(mesh):
    n_a = mesh.shape["ra"]
    n_c = mesh.shape["cb"]
    n_z = n_c // 2

    def peer(i, s, n):
        return i ^ s if n & (n - 1) == 0 else (i + s) % n

    def source(i, s, n):
        return i ^ s if n & (n - 1) == 0 else (i - s) % n

    def send_a(value, s):
        return lax.ppermute(value, "ra", [(i, peer(i, s, n_a)) for i in range(n_a)])

    def send_z(value, s):
        pairs = [(z * 2 + k, peer(z, s, n_z) * 2 + k) for z in range(n_z) for k in range(2)]
        return lax.ppermute(value, "cb", pairs)

    def send_core(value):
        return lax.ppermute(value, "cb", [(i, i ^ 1) for i in range(n_c)])

    def body(tokens, norm_gain, gate_weight, value_weight, gate_taps, value_taps, down_weight):
        layers, width, units = gate_weight.shape
        kernel = gate_taps.shape[1]
        count = tokens.shape[0]
        piece = -(-(-(-units // n_a)) // 8) * 8
        step = -(-(-(-piece // SPLITS)) // 8) * 8
        cuts = [(lo, min(step, piece - lo)) for lo in range(0, piece, step)]
        n_h = len(cuts)
        even = n_a * piece == units
        a = lax.axis_index("ra")
        c = lax.axis_index("cb")
        half = count // 2
        span = half // n_z

        def begin(p):
            return jnp.minimum(p * piece, units - piece)

        def scalar(value):
            return value.astype(jnp.int32).reshape(1)

        me_a, me_c = scalar(a), scalar(c)

        def stay(value):
            return pltpu.with_memory_space_constraint(value, pltpu.HBM)

        gate_rows = stay(gate_weight.transpose(0, 2, 1))
        value_rows = stay(value_weight.transpose(0, 2, 1))
        down_rows = stay(down_weight)

        tap_rows = 2 * kernel * layers
        tap_rows += -tap_rows % 8
        tap_args = [gate_taps.transpose(1, 0, 2), value_taps.transpose(1, 0, 2)]

        sends = list(range(n_a - 1, 0, -1))
        order = [(h, s) for h in range(n_h) for s in sends] + [(h, 0) for h in range(n_h)]

        def up(layer, pieces, held):
            outs = {}
            extra = None
            n_p = len(pieces)
            for h, s in order:
                lo, size = cuts[h]
                rows = 2 * size + (EXTRA if h == 0 else 0)
                initial = extra is None
                load = initial and held is None

                def body_fn(*refs, s=s, h=h, lo=lo, size=size, initial=initial, load=load):
                    a_ref, weights = refs[0], list(refs[1:3])
                    at = pl.ds(aligned(begin(peer(a_ref[0], s, n_a)) + lo), size)
                    if load:
                        sem, stored = refs[-1], refs[-4:-2]
                        ahead = begin(peer(a_ref[0], s, n_a))
                        blocks = [pl.ds(aligned(ahead), piece)]
                        for t in range(n_a):
                            if t != s:
                                blocks.append(pl.ds(aligned(begin(peer(a_ref[0], t, n_a))), piece))
                        if not even:
                            blocks = [slice(None)]
                        copies = []
                        for i, block in enumerate(blocks):
                            for k in range(2):
                                copy = pltpu.make_async_copy(
                                    weights[k].at[layer, block], stored[k].at[block], sem.at[2 * i + k]
                                )
                                copy.start()
                                copies.append(copy)
                        weights = stored
                    if initial:
                        sources = refs[3 : 3 + n_p]
                        gain_ref, side_ref = refs[3 + n_p : 5 + n_p]
                        out_ref, scaled_ref, tail_ref = refs[5 + n_p : 8 + n_p]
                        rows_ref = refs[-2] if load else refs[-1]
                        current = load_rows(sources, side_ref, rows_ref)
                        prepare(current, gain_ref[layer : layer + 1, :], scaled_ref, tail_ref)
                    else:
                        scaled_ref, tail_ref, out_ref = refs[3:6]
                    scaled = scaled_ref[...]
                    for k in range(2):
                        if load:
                            copies[k].wait()
                        out_ref[k * size : (k + 1) * size, :] = lax.dot_general(
                            weights[k][at, :],
                            scaled,
                            (((1,), (1,)), ((), ())),
                            preferred_element_type=F32,
                        ).astype(BF16)
                    if h == 0:
                        out_ref[2 * size : 2 * size + EXTRA, :] = tail_ref[...]
                    if load:
                        for copy in copies[2:]:
                            copy.wait()

                if load:
                    args, specs = [me_a, gate_rows, value_rows], [SMEM, HBM, HBM]
                else:
                    args, specs = [me_a, *held], [SMEM, VMEM, VMEM]
                shapes = [((rows, count), BF16)]
                scratch = []
                if initial:
                    args += [*pieces, norm_gain, me_c]
                    specs += [VMEM] * (n_p + 1) + [SMEM]
                    shapes += [((count, width), BF16), ((EXTRA, count), BF16)]
                    scratch = [pltpu.VMEM((count, width), BF16)]
                    if load:
                        shapes += [((units, width), BF16)] * 2
                        scratch += [pltpu.SemaphoreType.DMA((2 * n_a,))]
                else:
                    args += extra
                    specs += [VMEM] * 2
                out = call(
                    body_fn,
                    args,
                    specs,
                    shapes,
                    4 * size * width * count,
                    4 * size * width,
                    scratch,
                    room=WIDE if load else 16,
                )
                if initial:
                    extra = out[1:3]
                if load:
                    held = out[3:5]
                outs[h, s] = out[0]
            return outs

        def fetch(layer, after):
            sources, picks = [down_rows], [layer]
            if layer + 1 < layers:
                sources += [gate_rows, value_rows]
                picks += [layer + 1] * 2
            n = len(sources)
            shapes = [(source.shape[1:], BF16) for source in sources]
            args, specs = [*sources, after], [HBM] * n + [VMEM]
            scratch = [pltpu.SemaphoreType.DMA((n,))]
            if layer == 0:
                args += [me_a, *tap_args]
                specs += [SMEM, VMEM, VMEM]
                shapes.append(((piece, tap_rows), F32))
                scratch.append(pltpu.VMEM((units, tap_rows), F32))

            def body_fn(*refs):
                outs = refs[len(args) : len(args) + len(shapes)]
                sem = refs[len(args) + len(shapes)]
                copies = []
                for k in range(n):
                    copy = pltpu.make_async_copy(refs[k].at[picks[k]], outs[k], sem.at[k])
                    copy.start()
                    copies.append(copy)
                if layer == 0:
                    a_ref, gate_ref, value_ref = refs[n + 1 : n + 4]
                    rows = []
                    for l in range(layers):
                        for ref in (gate_ref, value_ref):
                            rows += [ref[k, l : l + 1, :] for k in range(kernel)]
                    if tap_rows > len(rows):
                        rows.append(jnp.zeros((tap_rows - len(rows), units), F32))
                    held_ref = refs[-1]
                    held_ref[...] = jnp.concatenate(rows, axis=0).T
                    outs[n][...] = held_ref[pl.ds(aligned(begin(a_ref[0])), piece), :]
                for copy in copies:
                    copy.wait()

            return call(
                body_fn,
                args,
                specs,
                shapes,
                2 * units * width * count,
                2 * n * units * width,
                scratch,
            )

        def act(layer, h, parts, inverse, taps):
            lo, size = cuts[h]
            first, last = h == 0, h == n_h - 1
            args = [*parts, taps] + ([] if first else [inverse])
            shapes = [((size, count), BF16)]
            if first and not last:
                shapes.append(((8, count), F32))

            def body_fn(*refs):
                parts_refs, taps_ref = refs[:n_a], refs[n_a]
                out_ref = refs[len(args)]
                total = parts_refs[0][...].astype(F32)
                for ref in parts_refs[1:]:
                    total = total + ref[...].astype(F32)
                if first:
                    tail = total[2 * size :]
                    scale = lax.rsqrt((tail[0:1] + tail[1:2]) / (width * n_a) + epsilon)
                    if not last:
                        refs[len(args) + 1][...] = jnp.broadcast_to(scale, (8, count))
                else:
                    scale = refs[n_a + 1][0:1, :]
                lin = total[: 2 * size] * scale
                lane = lax.broadcasted_iota(jnp.int32, (size, count), 1)

                def conv(kind):
                    result = None
                    for k in range(kernel):
                        shift = kernel - 1 - k
                        column = (layer * 2 + kind) * kernel + k
                        moved = lin[kind * size : (kind + 1) * size]
                        if shift:
                            moved = jnp.where(lane < shift, 0.0, pltpu.roll(moved, shift, 1))
                        term = taps_ref[lo : lo + size, column : column + 1] * moved
                        result = term if result is None else result + term
                    return result

                gate, value = conv(0), conv(1)
                out_ref[...] = (gate / (1.0 + jnp.exp(-gate)) * value).astype(BF16)

            out = call(
                body_fn,
                args,
                [VMEM] * len(args),
                shapes,
                60 * 2 * size * count,
                4 * n_a * size * count,
            )
            return out[0], (out[1] if len(out) > 1 else inverse)

        def term_of(left, weight, keep):
            if keep is not None:
                row = lax.broadcasted_iota(jnp.int32, left.shape, 0)
                left = jnp.where(row >= keep, left.astype(F32), 0.0).astype(BF16)
            return lax.dot_general(
                left, weight, (((0,), (0,)), ((), ())), preferred_element_type=F32
            )

        def down_own(weight, mine):
            def body_fn(weight_ref, a_ref, *refs):
                total = None
                p = a_ref[0]
                for h, (lo, size) in enumerate(cuts):
                    at = pl.ds(aligned(begin(p) + lo), size)
                    keep = None if even else p * piece - begin(p) - lo
                    term = term_of(refs[h][...], weight_ref[at, :], keep)
                    total = term if total is None else total + term
                refs[n_h][...] = total

            return call(
                body_fn,
                [weight, me_a, *mine],
                [VMEM, SMEM] + [VMEM] * n_h,
                [((count, width), F32)],
                2 * piece * width * count,
                2 * piece * width,
            )[0]

        def down(h, weight, total, others):
            lo, size = cuts[h]
            last = h == n_h - 1
            n = len(others)
            shapes = [((count, width), F32)]
            if last:
                shapes = [((half, width), BF16), ((half, width), F32)]

            def body_fn(weight_ref, sum_ref, a_ref, side_ref, *refs):
                total = sum_ref[...]
                for s in range(1, n_a):
                    p = source(a_ref[0], s, n_a)
                    at = pl.ds(aligned(begin(p) + lo), size)
                    keep = None if even else p * piece - begin(p) - lo
                    total = total + term_of(refs[s - 1][...], weight_ref[at, :], keep)
                if not last:
                    refs[n][...] = total
                    return
                away_ref, kept_ref, hold_ref = refs[n:]
                hold_ref[...] = total
                side = side_ref[0] & 1
                away = hold_ref[pl.ds(aligned((1 - side) * half, half), half), :]
                away_ref[...] = away.astype(BF16)
                kept_ref[...] = hold_ref[pl.ds(aligned(side * half, half), half), :]

            return call(
                body_fn,
                [weight, total, me_a, me_c, *others],
                [VMEM] * 2 + [SMEM] * 2 + [VMEM] * n,
                shapes,
                2 * size * (n_a - 1) * width * count,
                2 * size * (n_a - 1) * width,
                [pltpu.VMEM((count, width), F32)] if last else (),
            )

        def deal(kept, came):
            def body_fn(kept_ref, came_ref, z_ref, *refs):
                for s in range(n_z):
                    at = pl.ds(aligned(peer(z_ref[0] >> 1, s, n_z) * span), span)
                    value = kept_ref[at, :] + came_ref[at, :].astype(F32)
                    refs[s][...] = value.astype(refs[s].dtype)

            return call(
                body_fn,
                [kept, came, me_c],
                [VMEM, VMEM, SMEM],
                [((span, width), F32 if s == 0 else BF16) for s in range(n_z)],
                4 * half * width,
                8 * half * width,
            )

        def settle(layer, own, others, old):
            def body_fn(own_ref, *refs):
                at_ref, old_ref, out_ref = refs[-3:]
                branch = own_ref[...]
                for ref in refs[:-3]:
                    branch = branch + ref[...].astype(F32)
                if layer == 0:
                    at = (at_ref[0] & 1) * half + (at_ref[0] >> 1) * span
                    before = old_ref[pl.ds(aligned(at), span), :].astype(F32)
                else:
                    before = old_ref[...].astype(F32)
                out_ref[...] = (0.5 * before + branch).astype(BF16)

            return call(
                body_fn,
                [own, *others, me_c, old],
                [VMEM] * (1 + len(others)) + [SMEM, VMEM],
                [((span, width), BF16)],
                8 * span * width,
                8 * span * width,
            )[0]

        def gather(parts):
            def body_fn(*refs):
                z_ref, out_ref = refs[n_z:]
                for s in range(n_z):
                    at = pl.ds(aligned(source(z_ref[0] >> 1, s, n_z) * span), span)
                    out_ref[at, :] = refs[s][...]

            return call(
                body_fn,
                [*parts, me_c],
                [VMEM] * n_z + [SMEM],
                [((half, width), BF16)],
                half * width,
                4 * half * width,
            )[0]

        pieces = [tokens]
        old = tokens
        held = None
        for layer in range(layers):
            outs = up(layer, pieces, held)
            weight, *held = fetch(layer, outs[n_h - 1, 0])
            if layer == 0:
                *held, taps = held
            inverse = None
            mine, others = [], []
            for h in range(n_h):
                parts = [outs[h, 0]]
                parts += [send_a(outs[h, s], s) for s in range(1, n_a)]
                hidden, inverse = act(layer, h, parts, inverse, taps)
                mine.append(hidden)
                others.append([send_a(hidden, s) for s in range(1, n_a)])
            total = down_own(weight, mine)
            for h in range(n_h):
                out = down(h, weight, total, others[h])
                total = out[0]
            away, kept = out
            dealt = deal(kept, send_core(away))
            came = [send_z(dealt[s], s) for s in range(1, n_z)]
            old = settle(layer, dealt[0], came, old)
            near = gather([old] + [send_z(old, s) for s in range(1, n_z)])
            pieces = [near, send_core(near)]

        def join(near_ref, far_ref, side_ref, out_ref):
            side = side_ref[0] & 1
            out_ref[pl.ds(aligned(side * half, half), half), :] = near_ref[...]
            out_ref[pl.ds(aligned((1 - side) * half, half), half), :] = far_ref[...]

        return call(
            join,
            [*pieces, me_c],
            [VMEM, VMEM, SMEM],
            [((count, width), BF16)],
            count * width,
            4 * count * width,
        )[0]

    return body


def solution(mesh):
    return jax.shard_map(
        make_body(mesh),
        mesh=mesh,
        in_specs=(
            P(None, "ra"),
            P(None, "ra"),
            P(None, "ra", "cb"),
            P(None, "ra", "cb"),
            P(None, None, "cb"),
            P(None, None, "cb"),
            P(None, "cb", "ra"),
        ),
        out_specs=P(None, "ra"),
        check_vma=False,
    )
```

```python
import jax
import jax.numpy as jnp
from jax import lax
from jax.experimental import pallas as pl
from jax.experimental.pallas import tpu as pltpu
from jax.sharding import PartitionSpec as P


epsilon = 1e-06
F32 = jnp.float32
BF16 = jnp.bfloat16
EXTRA = 8
SPLITS = 2
MIB = 1 << 20
VMEM = pl.BlockSpec(memory_space=pltpu.VMEM)
SMEM = pl.BlockSpec(memory_space=pltpu.SMEM)
HBM = pl.BlockSpec(memory_space=pltpu.HBM)


def piece_of(units, members):
    return -(-(-(-units // members)) // 8) * 8


def splits_of(piece):
    return SPLITS if piece >= 128 else 1


def call(body, args, specs, shapes, flops, moved, scratch=(), room=16):
    return pl.pallas_call(
        body,
        in_specs=specs,
        out_specs=[VMEM] * len(shapes),
        out_shape=[jax.ShapeDtypeStruct(*shape) for shape in shapes],
        scratch_shapes=scratch,
        cost_estimate=pl.CostEstimate(
            flops=int(flops), bytes_accessed=int(moved), transcendentals=0
        ),
        compiler_params=pltpu.CompilerParams(vmem_limit_bytes=room * MIB),
    )(*args)


def aligned(value, step=8):
    return pl.multiple_of(value, step)


def prepare(current, gain, scaled_ref, tail_ref):
    scaled_ref[...] = (current * gain).astype(BF16)
    squares = current * current
    folded = squares[:, :128]
    for k in range(1, squares.shape[1] // 128):
        folded = folded + squares[:, k * 128 : (k + 1) * 128]
    total = jnp.sum(folded.T, axis=0, keepdims=True)
    high = total.astype(BF16).astype(F32)
    low = total - high
    row = lax.broadcasted_iota(jnp.int32, (EXTRA, total.shape[1]), 0)
    tail_ref[...] = jnp.where(row == 0, high, jnp.where(row == 1, low, 0.0)).astype(BF16)


def load_rows(pieces, side_ref, rows_ref):
    if len(pieces) == 1:
        return pieces[0][...].astype(F32)
    near, far = pieces
    half = near.shape[0]
    side = side_ref[0] & 1
    rows_ref[pl.ds(aligned(side * half, half), half), :] = near[...]
    rows_ref[pl.ds(aligned((1 - side) * half, half), half), :] = far[...]
    return rows_ref[...].astype(F32)


def make_body(mesh):
    n_a = mesh.shape["ra"]
    n_c = mesh.shape["cb"]
    n_z = n_c // 2

    def peer(i, s, n):
        return i ^ s if n & (n - 1) == 0 else (i + s) % n

    def source(i, s, n):
        return i ^ s if n & (n - 1) == 0 else (i - s) % n

    def send_a(value, s):
        return lax.ppermute(value, "ra", [(i, peer(i, s, n_a)) for i in range(n_a)])

    def send_z(value, s):
        pairs = [(z * 2 + k, peer(z, s, n_z) * 2 + k) for z in range(n_z) for k in range(2)]
        return lax.ppermute(value, "cb", pairs)

    def send_core(value):
        return lax.ppermute(value, "cb", [(i, i ^ 1) for i in range(n_c)])

    def body(tokens, norm_gain, gate_weight, value_weight, gate_taps, value_taps, down_weight):
        layers, width, units = gate_weight.shape
        kernel = gate_taps.shape[1]
        count = tokens.shape[0]
        piece = piece_of(units, n_a)
        splits = splits_of(piece)
        step = -(-(-(-piece // splits)) // 8) * 8
        cuts = [(lo, min(step, piece - lo)) for lo in range(0, piece, step)]
        n_h = len(cuts)
        even = n_a * piece == units
        a = lax.axis_index("ra")
        c = lax.axis_index("cb")
        half = count // 2
        span = half // n_z

        def begin(p):
            return jnp.minimum(p * piece, units - piece)

        def scalar(value):
            return value.astype(jnp.int32).reshape(1)

        me_a, me_c = scalar(a), scalar(c)

        def stay(value):
            return pltpu.with_memory_space_constraint(value, pltpu.HBM)

        gate_rows = stay(gate_weight.transpose(0, 2, 1))
        value_rows = stay(value_weight.transpose(0, 2, 1))
        down_rows = stay(down_weight)

        tap_rows = 2 * kernel * layers
        tap_rows += -tap_rows % 8
        tap_args = [gate_taps.transpose(1, 0, 2), value_taps.transpose(1, 0, 2)]

        sends = list(range(n_a - 1, 0, -1))
        order = [(h, s) for h in range(n_h) for s in sends] + [(h, 0) for h in range(n_h)]

        def up(layer, pieces, held):
            outs = {}
            extra = taps = None
            n_p = len(pieces)
            cold = held is None
            for index, (h, s) in enumerate(order):
                lo, size = cuts[h]
                rows = 2 * size + (EXTRA if h == 0 else 0)
                initial = index == 0
                load = cold and index == 1
                args = [me_a, *(held or (gate_rows, value_rows))]
                specs = [SMEM] + [VMEM if held else HBM] * 2
                shapes = [((rows, count), BF16)]
                scratch = []
                if initial and cold:
                    args += [stay(pieces[0]), stay(norm_gain), me_c]
                    specs += [HBM, HBM, SMEM]
                elif initial:
                    args += [*pieces, norm_gain, me_c]
                    specs += [VMEM] * (n_p + 1) + [SMEM]
                else:
                    args += extra
                    specs += [VMEM] * 2
                if initial:
                    shapes += [((count, width), BF16), ((EXTRA, count), BF16)]
                    scratch.append(pltpu.VMEM((count, width), BF16))
                if initial and cold:
                    scratch += [
                        pltpu.VMEM(norm_gain.shape, F32),
                        pltpu.VMEM((2, size, width), BF16),
                        pltpu.SemaphoreType.DMA((4,)),
                    ]
                if load:
                    args += [stay(value) for value in tap_args]
                    specs += [HBM, HBM]
                    shapes += [((units, width), BF16)] * 2 + [((piece, tap_rows), F32)]
                    scratch += [
                        pltpu.VMEM((2, *tap_args[0].shape), F32),
                        pltpu.VMEM((units, tap_rows), F32),
                        pltpu.SemaphoreType.DMA((2 * n_a + 2,)),
                    ]

                def body_fn(
                    *refs, s=s, lo=lo, size=size, h=h, initial=initial, load=load, n=len(args)
                ):
                    a_ref, gate_ref, value_ref = refs[:3]
                    weights = [gate_ref, value_ref]
                    out_ref = refs[n]
                    at = pl.ds(aligned(begin(peer(a_ref[0], s, n_a)) + lo), size)
                    waits = [(), ()]
                    copies = []

                    def launch(source_ref, target_ref, sem):
                        copy = pltpu.make_async_copy(source_ref, target_ref, sem)
                        copy.start()
                        return copy

                    if initial and cold:
                        rows_ref, gain_ref, block_ref, sem = refs[n + 3 :]
                        first = [
                            launch(refs[3], rows_ref, sem.at[0]),
                            launch(refs[4], gain_ref, sem.at[1]),
                        ]
                        for k in range(2):
                            waits[k] = (
                                launch(weights[k].at[layer, at], block_ref.at[k], sem.at[2 + k]),
                            )
                        for copy in first:
                            copy.wait()
                        current = rows_ref[...].astype(F32)
                        lefts = [block_ref.at[0], block_ref.at[1]]
                    elif load:
                        stored, taps_ref = refs[n + 1 : n + 3], refs[n + 3]
                        raw_ref, turned_ref, sem = refs[n + 4 :]
                        raw = [
                            launch(refs[5 + k], raw_ref.at[k], sem.at[2 * n_a + k]) for k in range(2)
                        ]
                        blocks = [slice(None)]
                        if even:
                            targets = [s] + [t for t in range(n_a) if t != s]
                            blocks = [
                                pl.ds(aligned(begin(peer(a_ref[0], t, n_a))), piece)
                                for t in targets
                            ]
                        for i, block in enumerate(blocks):
                            for k in range(2):
                                copies.append(
                                    launch(
                                        weights[k].at[layer, block],
                                        stored[k].at[block],
                                        sem.at[2 * i + k],
                                    )
                                )
                        waits = [(copies[0],), (copies[1],)]
                        copies = copies[2:]
                        lefts = [ref.at[at] for ref in stored]
                    else:
                        lefts = [ref.at[at] for ref in weights]
                        if initial:
                            gain_ref, side_ref = refs[3 + n_p : 5 + n_p]
                            current = load_rows(refs[3 : 3 + n_p], side_ref, refs[n + 3])
                    if initial:
                        scaled_ref, tail_ref = refs[n + 1 : n + 3]
                        prepare(current, gain_ref[layer : layer + 1, :], scaled_ref, tail_ref)
                    else:
                        scaled_ref, tail_ref = refs[3:5]
                    scaled = scaled_ref[...]
                    for k in range(2):
                        for copy in waits[k]:
                            copy.wait()
                        out_ref[k * size : (k + 1) * size, :] = lax.dot_general(
                            lefts[k][...],
                            scaled,
                            (((1,), (1,)), ((), ())),
                            preferred_element_type=F32,
                        ).astype(BF16)
                    if h == 0:
                        out_ref[2 * size : 2 * size + EXTRA, :] = tail_ref[...]
                    if load:
                        for copy in raw:
                            copy.wait()
                        lines = [
                            raw_ref[kind, k, l : l + 1, :]
                            for l in range(layers)
                            for kind in range(2)
                            for k in range(kernel)
                        ]
                        if tap_rows > len(lines):
                            lines.append(jnp.zeros((tap_rows - len(lines), units), F32))
                        turned_ref[...] = jnp.concatenate(lines, axis=0).T
                        taps_ref[...] = turned_ref[pl.ds(aligned(begin(a_ref[0])), piece), :]
                    for copy in copies:
                        copy.wait()

                out = call(
                    body_fn,
                    args,
                    specs,
                    shapes,
                    4 * size * width * count,
                    4 * size * width,
                    scratch,
                )
                if initial:
                    extra = out[1:3]
                if load:
                    held, taps = out[1:3], out[3]
                outs[h, s] = out[0]
            return outs, taps

        def fetch(layer, sources, after):
            n = len(sources)

            def body_fn(*refs):
                sem = refs[-1]
                copies = []
                for k in range(n):
                    copy = pltpu.make_async_copy(refs[k].at[layer], refs[n + 1 + k], sem.at[k])
                    copy.start()
                    copies.append(copy)
                for copy in copies:
                    copy.wait()

            return call(
                body_fn,
                [*sources, after],
                [HBM] * n + [VMEM],
                [(source.shape[1:], BF16) for source in sources],
                2 * units * width * count // 3 * n,
                2 * n * units * width,
                [pltpu.SemaphoreType.DMA((n,))],
            )

        def act(layer, h, parts, inverse, taps):
            lo, size = cuts[h]
            first, last = h == 0, h == n_h - 1
            args = [*parts, taps] + ([] if first else [inverse])
            shapes = [((size, count), BF16)]
            if first and not last:
                shapes.append(((8, count), F32))

            def body_fn(*refs):
                parts_refs, taps_ref = refs[:n_a], refs[n_a]
                out_ref = refs[len(args)]
                total = parts_refs[0][...].astype(F32)
                for ref in parts_refs[1:]:
                    total = total + ref[...].astype(F32)
                if first:
                    tail = total[2 * size :]
                    scale = lax.rsqrt((tail[0:1] + tail[1:2]) / (width * n_a) + epsilon)
                    if not last:
                        refs[len(args) + 1][...] = jnp.broadcast_to(scale, (8, count))
                else:
                    scale = refs[n_a + 1][0:1, :]
                lin = total[: 2 * size] * scale
                lane = lax.broadcasted_iota(jnp.int32, (size, count), 1)

                def conv(kind):
                    result = None
                    for k in range(kernel):
                        shift = kernel - 1 - k
                        column = (layer * 2 + kind) * kernel + k
                        moved = lin[kind * size : (kind + 1) * size]
                        if shift:
                            moved = jnp.where(lane < shift, 0.0, pltpu.roll(moved, shift, 1))
                        term = taps_ref[lo : lo + size, column : column + 1] * moved
                        result = term if result is None else result + term
                    return result

                gate, value = conv(0), conv(1)
                out_ref[...] = (gate / (1.0 + jnp.exp(-gate)) * value).astype(BF16)

            out = call(
                body_fn,
                args,
                [VMEM] * len(args),
                shapes,
                60 * 2 * size * count,
                4 * n_a * size * count,
            )
            return out[0], (out[1] if len(out) > 1 else inverse)

        def term_of(left, weight, keep):
            if keep is not None:
                row = lax.broadcasted_iota(jnp.int32, left.shape, 0)
                left = jnp.where(row >= keep, left.astype(F32), 0.0).astype(BF16)
            return lax.dot_general(
                left, weight, (((0,), (0,)), ((), ())), preferred_element_type=F32
            )

        def down_own(weight, mine):
            def body_fn(weight_ref, a_ref, *refs):
                total = None
                p = a_ref[0]
                for h, (lo, size) in enumerate(cuts):
                    at = pl.ds(aligned(begin(p) + lo), size)
                    keep = None if even else p * piece - begin(p) - lo
                    term = term_of(refs[h][...], weight_ref[at, :], keep)
                    total = term if total is None else total + term
                refs[n_h][...] = total

            return call(
                body_fn,
                [weight, me_a, *mine],
                [VMEM, SMEM] + [VMEM] * n_h,
                [((count, width), F32)],
                2 * piece * width * count,
                2 * piece * width,
            )[0]

        def down(h, weight, total, others):
            lo, size = cuts[h]
            last = h == n_h - 1
            n = len(others)
            shapes = [((count, width), F32)]
            if last:
                shapes = [((half, width), BF16), ((half, width), F32)]

            def body_fn(weight_ref, sum_ref, a_ref, side_ref, *refs):
                total = sum_ref[...]
                for s in range(1, n_a):
                    p = source(a_ref[0], s, n_a)
                    at = pl.ds(aligned(begin(p) + lo), size)
                    keep = None if even else p * piece - begin(p) - lo
                    total = total + term_of(refs[s - 1][...], weight_ref[at, :], keep)
                if not last:
                    refs[n][...] = total
                    return
                away_ref, kept_ref, hold_ref = refs[n:]
                hold_ref[...] = total
                side = side_ref[0] & 1
                away = hold_ref[pl.ds(aligned((1 - side) * half, half), half), :]
                away_ref[...] = away.astype(BF16)
                kept_ref[...] = hold_ref[pl.ds(aligned(side * half, half), half), :]

            return call(
                body_fn,
                [weight, total, me_a, me_c, *others],
                [VMEM] * 2 + [SMEM] * 2 + [VMEM] * n,
                shapes,
                2 * size * (n_a - 1) * width * count,
                2 * size * (n_a - 1) * width,
                [pltpu.VMEM((count, width), F32)] if last else (),
            )

        def deal(kept, came):
            def body_fn(kept_ref, came_ref, z_ref, *refs):
                for s in range(n_z):
                    at = pl.ds(aligned(peer(z_ref[0] >> 1, s, n_z) * span), span)
                    value = kept_ref[at, :] + came_ref[at, :].astype(F32)
                    refs[s][...] = value.astype(refs[s].dtype)

            return call(
                body_fn,
                [kept, came, me_c],
                [VMEM, VMEM, SMEM],
                [((span, width), F32 if s == 0 else BF16) for s in range(n_z)],
                4 * half * width,
                8 * half * width,
            )

        def settle(layer, own, others, old):
            def body_fn(own_ref, *refs):
                at_ref, old_ref, out_ref = refs[-3:]
                branch = own_ref[...]
                for ref in refs[:-3]:
                    branch = branch + ref[...].astype(F32)
                if layer == 0:
                    at = (at_ref[0] & 1) * half + (at_ref[0] >> 1) * span
                    before = old_ref[pl.ds(aligned(at), span), :].astype(F32)
                else:
                    before = old_ref[...].astype(F32)
                out_ref[...] = (0.5 * before + branch).astype(BF16)

            return call(
                body_fn,
                [own, *others, me_c, old],
                [VMEM] * (1 + len(others)) + [SMEM, VMEM],
                [((span, width), BF16)],
                8 * span * width,
                8 * span * width,
            )[0]

        def gather(parts):
            def body_fn(*refs):
                z_ref, out_ref = refs[n_z:]
                for s in range(n_z):
                    at = pl.ds(aligned(source(z_ref[0] >> 1, s, n_z) * span), span)
                    out_ref[at, :] = refs[s][...]

            return call(
                body_fn,
                [*parts, me_c],
                [VMEM] * n_z + [SMEM],
                [((half, width), BF16)],
                half * width,
                4 * half * width,
            )[0]

        pieces = [tokens]
        old = tokens
        held = taps = None
        for layer in range(layers):
            outs, came_taps = up(layer, pieces, held)
            taps = taps if came_taps is None else came_taps
            (weight,) = fetch(layer, [down_rows], outs[n_h - 1, 0])
            inverse = None
            mine, others = [], []
            for h in range(n_h):
                parts = [outs[h, 0]]
                parts += [send_a(outs[h, s], s) for s in range(1, n_a)]
                hidden, inverse = act(layer, h, parts, inverse, taps)
                mine.append(hidden)
                others.append([send_a(hidden, s) for s in range(1, n_a)])
            total = down_own(weight, mine)
            for h in range(n_h):
                out = down(h, weight, total, others[h])
                total = out[0]
            away, kept = out
            dealt = deal(kept, send_core(away))
            came = [send_z(dealt[s], s) for s in range(1, n_z)]
            if layer + 1 < layers:
                ahead = [gate_rows, value_rows]
                held = fetch(layer + 1, ahead, dealt[0])
            old = settle(layer, dealt[0], came, old)
            near = gather([old] + [send_z(old, s) for s in range(1, n_z)])
            pieces = [near, send_core(near)]

        def join(near_ref, far_ref, side_ref, out_ref):
            side = side_ref[0] & 1
            out_ref[pl.ds(aligned(side * half, half), half), :] = near_ref[...]
            out_ref[pl.ds(aligned((1 - side) * half, half), half), :] = far_ref[...]

        return call(
            join,
            [*pieces, me_c],
            [VMEM, VMEM, SMEM],
            [((count, width), BF16)],
            count * width,
            4 * count * width,
        )[0]

    return body


def solution(mesh):
    return jax.shard_map(
        make_body(mesh),
        mesh=mesh,
        in_specs=(
            P(None, "ra"),
            P(None, "ra"),
            P(None, "ra", "cb"),
            P(None, "ra", "cb"),
            P(None, None, "cb"),
            P(None, None, "cb"),
            P(None, "cb", "ra"),
        ),
        out_specs=P(None, "ra"),
        check_vma=False,
    )
```

```python
import jax
import jax.numpy as jnp
from jax import lax
from jax.experimental import pallas as pl
from jax.experimental.pallas import tpu as pltpu
from jax.sharding import PartitionSpec as P


epsilon = 1e-06
F32 = jnp.float32
BF16 = jnp.bfloat16
EXTRA = 8
SPLITS = 2
MIB = 1 << 20
VMEM = pl.BlockSpec(memory_space=pltpu.VMEM)
SMEM = pl.BlockSpec(memory_space=pltpu.SMEM)
HBM = pl.BlockSpec(memory_space=pltpu.HBM)


def piece_of(units, members):
    return -(-(-(-units // members)) // 8) * 8


def splits_of(piece):
    return SPLITS if piece >= 128 else 1


def call(body, args, specs, shapes, flops, moved, scratch=(), room=16):
    return pl.pallas_call(
        body,
        in_specs=specs,
        out_specs=[VMEM] * len(shapes),
        out_shape=[jax.ShapeDtypeStruct(*shape) for shape in shapes],
        scratch_shapes=scratch,
        cost_estimate=pl.CostEstimate(
            flops=int(flops), bytes_accessed=int(moved), transcendentals=0
        ),
        compiler_params=pltpu.CompilerParams(vmem_limit_bytes=room * MIB),
    )(*args)


def aligned(value, step=8):
    return pl.multiple_of(value, step)


def prepare(current, gain, scaled_ref, tail_ref):
    scaled_ref[...] = (current * gain).astype(BF16)
    squares = current * current
    folded = squares[:, :128]
    for k in range(1, squares.shape[1] // 128):
        folded = folded + squares[:, k * 128 : (k + 1) * 128]
    total = jnp.sum(folded.T, axis=0, keepdims=True)
    high = total.astype(BF16).astype(F32)
    low = total - high
    row = lax.broadcasted_iota(jnp.int32, (EXTRA, total.shape[1]), 0)
    tail_ref[...] = jnp.where(row == 0, high, jnp.where(row == 1, low, 0.0)).astype(BF16)


def load_rows(pieces, side_ref, rows_ref):
    if len(pieces) == 1:
        return pieces[0][...].astype(F32)
    near, far = pieces
    half = near.shape[0]
    side = side_ref[0] & 1
    rows_ref[pl.ds(aligned(side * half, half), half), :] = near[...]
    rows_ref[pl.ds(aligned((1 - side) * half, half), half), :] = far[...]
    return rows_ref[...].astype(F32)


def make_body(mesh):
    n_a = mesh.shape["ra"]
    n_c = mesh.shape["cb"]
    n_z = n_c // 2

    def peer(i, s, n):
        return i ^ s if n & (n - 1) == 0 else (i + s) % n

    def source(i, s, n):
        return i ^ s if n & (n - 1) == 0 else (i - s) % n

    def send_a(value, s):
        return lax.ppermute(value, "ra", [(i, peer(i, s, n_a)) for i in range(n_a)])

    def send_z(value, s):
        pairs = [(z * 2 + k, peer(z, s, n_z) * 2 + k) for z in range(n_z) for k in range(2)]
        return lax.ppermute(value, "cb", pairs)

    def send_core(value):
        return lax.ppermute(value, "cb", [(i, i ^ 1) for i in range(n_c)])

    def body(tokens, norm_gain, gate_weight, value_weight, gate_taps, value_taps, down_weight):
        layers, width, units = gate_weight.shape
        kernel = gate_taps.shape[1]
        count = tokens.shape[0]
        piece = piece_of(units, n_a)
        splits = splits_of(piece)
        step = piece if splits == 1 else -(-2 * piece // 24) * 8
        cuts = [(lo, min(step, piece - lo)) for lo in range(0, piece, step)]
        n_h = len(cuts)
        even = n_a * piece == units
        a = lax.axis_index("ra")
        c = lax.axis_index("cb")
        half = count // 2
        span = half // n_z

        def begin(p):
            return jnp.minimum(p * piece, units - piece)

        def scalar(value):
            return value.astype(jnp.int32).reshape(1)

        me_a, me_c = scalar(a), scalar(c)

        def stay(value):
            return pltpu.with_memory_space_constraint(value, pltpu.HBM)

        gate_rows = stay(gate_weight.transpose(0, 2, 1))
        value_rows = stay(value_weight.transpose(0, 2, 1))
        down_rows = stay(down_weight)

        tap_rows = 2 * kernel * layers
        tap_rows += -tap_rows % 8
        tap_args = [gate_taps.transpose(1, 0, 2), value_taps.transpose(1, 0, 2)]

        sends = list(range(n_a - 1, 0, -1))
        order = [(h, s) for h in range(n_h) for s in sends] + [(h, 0) for h in range(n_h)]

        def up(layer, pieces, held):
            outs = {}
            extra = taps = None
            n_p = len(pieces)
            cold = held is None
            for index, (h, s) in enumerate(order):
                lo, size = cuts[h]
                rows = 2 * size + (EXTRA if h == 0 else 0)
                initial = index == 0
                load = cold and index == 1
                args = [me_a, *(held or (gate_rows, value_rows))]
                specs = [SMEM] + [VMEM if held else HBM] * 2
                shapes = [((rows, count), BF16)]
                scratch = []
                if initial and cold:
                    args += [stay(pieces[0]), stay(norm_gain), me_c]
                    specs += [HBM, HBM, SMEM]
                elif initial:
                    args += [*pieces, norm_gain, me_c]
                    specs += [VMEM] * (n_p + 1) + [SMEM]
                else:
                    args += extra
                    specs += [VMEM] * 2
                if initial:
                    shapes += [((count, width), BF16), ((EXTRA, count), BF16)]
                    scratch.append(pltpu.VMEM((count, width), BF16))
                if initial and cold:
                    scratch += [
                        pltpu.VMEM(norm_gain.shape, F32),
                        pltpu.VMEM((2, size, width), BF16),
                        pltpu.SemaphoreType.DMA((4,)),
                    ]
                if load:
                    args += [stay(value) for value in tap_args]
                    specs += [HBM, HBM]
                    shapes += [((units, width), BF16)] * 2 + [((piece, tap_rows), F32)]
                    scratch += [
                        pltpu.VMEM((2, *tap_args[0].shape), F32),
                        pltpu.VMEM((units, tap_rows), F32),
                        pltpu.SemaphoreType.DMA((2 * n_a + 2,)),
                    ]

                def body_fn(
                    *refs, s=s, lo=lo, size=size, h=h, initial=initial, load=load, n=len(args)
                ):
                    a_ref, gate_ref, value_ref = refs[:3]
                    weights = [gate_ref, value_ref]
                    out_ref = refs[n]
                    at = pl.ds(aligned(begin(peer(a_ref[0], s, n_a)) + lo), size)
                    waits = [(), ()]
                    copies = []

                    def launch(source_ref, target_ref, sem):
                        copy = pltpu.make_async_copy(source_ref, target_ref, sem)
                        copy.start()
                        return copy

                    if initial and cold:
                        rows_ref, gain_ref, block_ref, sem = refs[n + 3 :]
                        first = [
                            launch(refs[3], rows_ref, sem.at[0]),
                            launch(refs[4], gain_ref, sem.at[1]),
                        ]
                        for k in range(2):
                            waits[k] = (
                                launch(weights[k].at[layer, at], block_ref.at[k], sem.at[2 + k]),
                            )
                        for copy in first:
                            copy.wait()
                        current = rows_ref[...].astype(F32)
                        lefts = [block_ref.at[0], block_ref.at[1]]
                    elif load:
                        stored, taps_ref = refs[n + 1 : n + 3], refs[n + 3]
                        raw_ref, turned_ref, sem = refs[n + 4 :]
                        raw = [
                            launch(refs[5 + k], raw_ref.at[k], sem.at[2 * n_a + k]) for k in range(2)
                        ]
                        blocks = [slice(None)]
                        if even:
                            targets = [s] + [t for t in range(n_a) if t != s]
                            blocks = [
                                pl.ds(aligned(begin(peer(a_ref[0], t, n_a))), piece)
                                for t in targets
                            ]
                        for i, block in enumerate(blocks):
                            for k in range(2):
                                copies.append(
                                    launch(
                                        weights[k].at[layer, block],
                                        stored[k].at[block],
                                        sem.at[2 * i + k],
                                    )
                                )
                        waits = [(copies[0],), (copies[1],)]
                        copies = copies[2:]
                        lefts = [ref.at[at] for ref in stored]
                    else:
                        lefts = [ref.at[at] for ref in weights]
                        if initial:
                            gain_ref, side_ref = refs[3 + n_p : 5 + n_p]
                            current = load_rows(refs[3 : 3 + n_p], side_ref, refs[n + 3])
                    if initial:
                        scaled_ref, tail_ref = refs[n + 1 : n + 3]
                        prepare(current, gain_ref[layer : layer + 1, :], scaled_ref, tail_ref)
                    else:
                        scaled_ref, tail_ref = refs[3:5]
                    scaled = scaled_ref[...]
                    for k in range(2):
                        for copy in waits[k]:
                            copy.wait()
                        out_ref[k * size : (k + 1) * size, :] = lax.dot_general(
                            lefts[k][...],
                            scaled,
                            (((1,), (1,)), ((), ())),
                            preferred_element_type=F32,
                        ).astype(BF16)
                    if h == 0:
                        out_ref[2 * size : 2 * size + EXTRA, :] = tail_ref[...]
                    if load:
                        for copy in raw:
                            copy.wait()
                        lines = [
                            raw_ref[kind, k, l : l + 1, :]
                            for l in range(layers)
                            for kind in range(2)
                            for k in range(kernel)
                        ]
                        if tap_rows > len(lines):
                            lines.append(jnp.zeros((tap_rows - len(lines), units), F32))
                        turned_ref[...] = jnp.concatenate(lines, axis=0).T
                        taps_ref[...] = turned_ref[pl.ds(aligned(begin(a_ref[0])), piece), :]
                    for copy in copies:
                        copy.wait()

                out = call(
                    body_fn,
                    args,
                    specs,
                    shapes,
                    4 * size * width * count,
                    4 * size * width,
                    scratch,
                )
                if initial:
                    extra = out[1:3]
                if load:
                    held, taps = out[1:3], out[3]
                outs[h, s] = out[0]
            return outs, taps

        def fetch(layer, sources, after):
            n = len(sources)

            def body_fn(*refs):
                sem = refs[-1]
                copies = []
                for k in range(n):
                    copy = pltpu.make_async_copy(refs[k].at[layer], refs[n + 1 + k], sem.at[k])
                    copy.start()
                    copies.append(copy)
                for copy in copies:
                    copy.wait()

            return call(
                body_fn,
                [*sources, after],
                [HBM] * n + [VMEM],
                [(source.shape[1:], BF16) for source in sources],
                2 * units * width * count // 3 * n,
                2 * n * units * width,
                [pltpu.SemaphoreType.DMA((n,))],
            )

        def act(layer, h, parts, inverse, taps):
            lo, size = cuts[h]
            first, last = h == 0, h == n_h - 1
            args = [*parts, taps] + ([] if first else [inverse])
            shapes = [((size, count), BF16)]
            if first and not last:
                shapes.append(((8, count), F32))

            def body_fn(*refs):
                parts_refs, taps_ref = refs[:n_a], refs[n_a]
                out_ref = refs[len(args)]
                total = parts_refs[0][...].astype(F32)
                for ref in parts_refs[1:]:
                    total = total + ref[...].astype(F32)
                if first:
                    tail = total[2 * size :]
                    scale = lax.rsqrt((tail[0:1] + tail[1:2]) / (width * n_a) + epsilon)
                    if not last:
                        refs[len(args) + 1][...] = jnp.broadcast_to(scale, (8, count))
                else:
                    scale = refs[n_a + 1][0:1, :]
                lin = total[: 2 * size] * scale
                lane = lax.broadcasted_iota(jnp.int32, (size, count), 1)

                def conv(kind):
                    result = None
                    for k in range(kernel):
                        shift = kernel - 1 - k
                        column = (layer * 2 + kind) * kernel + k
                        moved = lin[kind * size : (kind + 1) * size]
                        if shift:
                            moved = jnp.where(lane < shift, 0.0, pltpu.roll(moved, shift, 1))
                        term = taps_ref[lo : lo + size, column : column + 1] * moved
                        result = term if result is None else result + term
                    return result

                gate, value = conv(0), conv(1)
                out_ref[...] = (gate / (1.0 + jnp.exp(-gate)) * value).astype(BF16)

            out = call(
                body_fn,
                args,
                [VMEM] * len(args),
                shapes,
                60 * 2 * size * count,
                4 * n_a * size * count,
            )
            return out[0], (out[1] if len(out) > 1 else inverse)

        def term_of(left, weight, keep):
            if keep is not None:
                row = lax.broadcasted_iota(jnp.int32, left.shape, 0)
                left = jnp.where(row >= keep, left.astype(F32), 0.0).astype(BF16)
            return lax.dot_general(
                left, weight, (((0,), (0,)), ((), ())), preferred_element_type=F32
            )

        def down_own(weight, mine):
            def body_fn(weight_ref, a_ref, *refs):
                total = None
                p = a_ref[0]
                for h, (lo, size) in enumerate(cuts):
                    at = pl.ds(aligned(begin(p) + lo), size)
                    keep = None if even else p * piece - begin(p) - lo
                    term = term_of(refs[h][...], weight_ref[at, :], keep)
                    total = term if total is None else total + term
                refs[n_h][...] = total

            return call(
                body_fn,
                [weight, me_a, *mine],
                [VMEM, SMEM] + [VMEM] * n_h,
                [((count, width), F32)],
                2 * piece * width * count,
                2 * piece * width,
            )[0]

        def down(h, weight, total, others, picks, last):
            lo, size = cuts[h]
            n = len(picks)
            shapes = [((count, width), F32)]
            if last:
                shapes = [((half, width), BF16), ((half, width), F32)]

            def body_fn(weight_ref, sum_ref, a_ref, side_ref, *refs):
                total = sum_ref[...]
                for i, s in enumerate(picks):
                    p = source(a_ref[0], s, n_a)
                    at = pl.ds(aligned(begin(p) + lo), size)
                    keep = None if even else p * piece - begin(p) - lo
                    total = total + term_of(refs[i][...], weight_ref[at, :], keep)
                if not last:
                    refs[n][...] = total
                    return
                away_ref, kept_ref, hold_ref = refs[n:]
                hold_ref[...] = total
                side = side_ref[0] & 1
                away = hold_ref[pl.ds(aligned((1 - side) * half, half), half), :]
                away_ref[...] = away.astype(BF16)
                kept_ref[...] = hold_ref[pl.ds(aligned(side * half, half), half), :]

            return call(
                body_fn,
                [weight, total, me_a, me_c, *[others[s - 1] for s in picks]],
                [VMEM] * 2 + [SMEM] * 2 + [VMEM] * n,
                shapes,
                2 * size * n * width * count,
                2 * size * n * width,
                [pltpu.VMEM((count, width), F32)] if last else (),
            )

        def deal(kept, came):
            def body_fn(kept_ref, came_ref, z_ref, *refs):
                for s in range(n_z):
                    at = pl.ds(aligned(peer(z_ref[0] >> 1, s, n_z) * span), span)
                    value = kept_ref[at, :] + came_ref[at, :].astype(F32)
                    refs[s][...] = value.astype(refs[s].dtype)

            return call(
                body_fn,
                [kept, came, me_c],
                [VMEM, VMEM, SMEM],
                [((span, width), F32 if s == 0 else BF16) for s in range(n_z)],
                4 * half * width,
                8 * half * width,
            )

        def settle(layer, own, others, old):
            def body_fn(own_ref, *refs):
                at_ref, old_ref, out_ref = refs[-3:]
                branch = own_ref[...]
                for ref in refs[:-3]:
                    branch = branch + ref[...].astype(F32)
                if layer == 0:
                    at = (at_ref[0] & 1) * half + (at_ref[0] >> 1) * span
                    before = old_ref[pl.ds(aligned(at), span), :].astype(F32)
                else:
                    before = old_ref[...].astype(F32)
                out_ref[...] = (0.5 * before + branch).astype(BF16)

            return call(
                body_fn,
                [own, *others, me_c, old],
                [VMEM] * (1 + len(others)) + [SMEM, VMEM],
                [((span, width), BF16)],
                8 * span * width,
                8 * span * width,
            )[0]

        def gather(parts):
            def body_fn(*refs):
                z_ref, out_ref = refs[n_z:]
                for s in range(n_z):
                    at = pl.ds(aligned(source(z_ref[0] >> 1, s, n_z) * span), span)
                    out_ref[at, :] = refs[s][...]

            return call(
                body_fn,
                [*parts, me_c],
                [VMEM] * n_z + [SMEM],
                [((half, width), BF16)],
                half * width,
                4 * half * width,
            )[0]

        pieces = [tokens]
        old = tokens
        held = taps = None
        for layer in range(layers):
            outs, came_taps = up(layer, pieces, held)
            taps = taps if came_taps is None else came_taps
            (weight,) = fetch(layer, [down_rows], outs[n_h - 1, 0])
            inverse = None
            mine, others = [], []
            for h in range(n_h):
                parts = [outs[h, 0]]
                parts += [send_a(outs[h, s], s) for s in range(1, n_a)]
                hidden, inverse = act(layer, h, parts, inverse, taps)
                mine.append(hidden)
                others.append([send_a(hidden, s) for s in range(1, n_a)])
            total = down_own(weight, mine)
            turns = [(h, list(range(1, n_a))) for h in range(n_h)]
            if n_a == 4:
                turns = turns[:-1] + [(n_h - 1, [3, 1]), (n_h - 1, [2])]
            for i, (h, picks) in enumerate(turns):
                out = down(h, weight, total, others[h], picks, i == len(turns) - 1)
                total = out[0]
            away, kept = out
            dealt = deal(kept, send_core(away))
            came = [send_z(dealt[s], s) for s in range(1, n_z)]
            if layer + 1 < layers:
                ahead = [gate_rows, value_rows]
                held = fetch(layer + 1, ahead, dealt[0])
            old = settle(layer, dealt[0], came, old)
            near = gather([old] + [send_z(old, s) for s in range(1, n_z)])
            pieces = [near, send_core(near)]

        def join(near_ref, far_ref, side_ref, out_ref):
            side = side_ref[0] & 1
            out_ref[pl.ds(aligned(side * half, half), half), :] = near_ref[...]
            out_ref[pl.ds(aligned((1 - side) * half, half), half), :] = far_ref[...]

        return call(
            join,
            [*pieces, me_c],
            [VMEM, VMEM, SMEM],
            [((count, width), BF16)],
            count * width,
            4 * count * width,
        )[0]

    return body


def solution(mesh):
    return jax.shard_map(
        make_body(mesh),
        mesh=mesh,
        in_specs=(
            P(None, "ra"),
            P(None, "ra"),
            P(None, "ra", "cb"),
            P(None, "ra", "cb"),
            P(None, None, "cb"),
            P(None, None, "cb"),
            P(None, "cb", "ra"),
        ),
        out_specs=P(None, "ra"),
        check_vma=False,
    )
```

```python
import jax
import jax.numpy as jnp
from jax import lax
from jax.experimental import pallas as pl
from jax.experimental.pallas import tpu as pltpu
from jax.sharding import PartitionSpec as P


epsilon = 1e-06
F32 = jnp.float32
BF16 = jnp.bfloat16
EXTRA = 8
SPLITS = 2
MIB = 1 << 20
VMEM = pl.BlockSpec(memory_space=pltpu.VMEM)
SMEM = pl.BlockSpec(memory_space=pltpu.SMEM)
HBM = pl.BlockSpec(memory_space=pltpu.HBM)


def piece_of(units, members):
    return -(-(-(-units // members)) // 8) * 8


def splits_of(piece):
    return SPLITS if piece >= 128 else 1


def call(body, args, specs, shapes, flops, moved, scratch=(), room=16):
    return pl.pallas_call(
        body,
        in_specs=specs,
        out_specs=[VMEM] * len(shapes),
        out_shape=[jax.ShapeDtypeStruct(*shape) for shape in shapes],
        scratch_shapes=scratch,
        cost_estimate=pl.CostEstimate(
            flops=int(flops), bytes_accessed=int(moved), transcendentals=0
        ),
        compiler_params=pltpu.CompilerParams(vmem_limit_bytes=room * MIB),
    )(*args)


def aligned(value, step=8):
    return pl.multiple_of(value, step)


def prepare(current, gain, scaled_ref, tail_ref):
    scaled_ref[...] = (current * gain).astype(BF16)
    squares = current * current
    folded = squares[:, :128]
    for k in range(1, squares.shape[1] // 128):
        folded = folded + squares[:, k * 128 : (k + 1) * 128]
    total = jnp.sum(folded.T, axis=0, keepdims=True)
    high = total.astype(BF16).astype(F32)
    low = total - high
    row = lax.broadcasted_iota(jnp.int32, (EXTRA, total.shape[1]), 0)
    tail_ref[...] = jnp.where(row == 0, high, jnp.where(row == 1, low, 0.0)).astype(BF16)


def load_rows(pieces, side_ref, rows_ref):
    if len(pieces) == 1:
        return pieces[0][...].astype(F32)
    near, far = pieces
    half = near.shape[0]
    side = side_ref[0] & 1
    rows_ref[pl.ds(aligned(side * half, half), half), :] = near[...]
    rows_ref[pl.ds(aligned((1 - side) * half, half), half), :] = far[...]
    return rows_ref[...].astype(F32)


def make_body(mesh):
    n_a = mesh.shape["ra"]
    n_c = mesh.shape["cb"]
    n_z = n_c // 2

    def peer(i, s, n):
        return i ^ s if n & (n - 1) == 0 else (i + s) % n

    def source(i, s, n):
        return i ^ s if n & (n - 1) == 0 else (i - s) % n

    def send_a(value, s):
        return lax.ppermute(value, "ra", [(i, peer(i, s, n_a)) for i in range(n_a)])

    def send_z(value, s):
        pairs = [(z * 2 + k, peer(z, s, n_z) * 2 + k) for z in range(n_z) for k in range(2)]
        return lax.ppermute(value, "cb", pairs)

    def send_core(value):
        return lax.ppermute(value, "cb", [(i, i ^ 1) for i in range(n_c)])

    def body(tokens, norm_gain, gate_weight, value_weight, gate_taps, value_taps, down_weight):
        layers, width, units = gate_weight.shape
        kernel = gate_taps.shape[1]
        count = tokens.shape[0]
        piece = piece_of(units, n_a)
        splits = splits_of(piece)
        step = piece if splits == 1 else -(-2 * piece // 24) * 8
        cuts = [(lo, min(step, piece - lo)) for lo in range(0, piece, step)]
        n_h = len(cuts)
        even = n_a * piece == units
        a = lax.axis_index("ra")
        c = lax.axis_index("cb")
        half = count // 2
        span = half // n_z

        def begin(p):
            return jnp.minimum(p * piece, units - piece)

        def scalar(value):
            return value.astype(jnp.int32).reshape(1)

        me_a, me_c = scalar(a), scalar(c)

        def stay(value):
            return pltpu.with_memory_space_constraint(value, pltpu.HBM)

        gate_rows = stay(gate_weight.transpose(0, 2, 1))
        value_rows = stay(value_weight.transpose(0, 2, 1))
        down_rows = stay(down_weight)

        tap_rows = 2 * kernel * layers
        tap_rows += -tap_rows % 8
        tap_args = [gate_taps.transpose(1, 0, 2), value_taps.transpose(1, 0, 2)]

        sends = list(range(n_a - 1, 0, -1))
        order = [(h, s) for h in range(n_h) for s in sends] + [(h, 0) for h in range(n_h)]

        def up(layer, pieces, held):
            outs = {}
            extra = taps = None
            n_p = len(pieces)
            cold = held is None
            for index, (h, s) in enumerate(order):
                lo, size = cuts[h]
                rows = 2 * size + (EXTRA if h == 0 else 0)
                initial = index == 0
                load = cold and index == 1
                args = [me_a, *(held or (gate_rows, value_rows))]
                specs = [SMEM] + [VMEM if held else HBM] * 2
                shapes = [((rows, count), BF16)]
                scratch = []
                if initial and cold:
                    args += [stay(pieces[0]), stay(norm_gain), me_c]
                    specs += [HBM, HBM, SMEM]
                elif initial:
                    args += [*pieces, norm_gain, me_c]
                    specs += [VMEM] * (n_p + 1) + [SMEM]
                else:
                    args += extra
                    specs += [VMEM] * 2
                if initial:
                    shapes += [((count, width), BF16), ((EXTRA, count), BF16)]
                    scratch.append(pltpu.VMEM((count, width), BF16))
                if initial and cold:
                    scratch += [
                        pltpu.VMEM(norm_gain.shape, F32),
                        pltpu.VMEM((2, size, width), BF16),
                        pltpu.SemaphoreType.DMA((4,)),
                    ]
                if load:
                    args += [stay(value) for value in tap_args]
                    specs += [HBM, HBM]
                    shapes += [((units, width), BF16)] * 2 + [((piece, tap_rows), F32)]
                    scratch += [
                        pltpu.VMEM((2, *tap_args[0].shape), F32),
                        pltpu.VMEM((units, tap_rows), F32),
                        pltpu.SemaphoreType.DMA((2 * n_a + 2,)),
                    ]

                def body_fn(
                    *refs, s=s, lo=lo, size=size, h=h, initial=initial, load=load, n=len(args)
                ):
                    a_ref, gate_ref, value_ref = refs[:3]
                    weights = [gate_ref, value_ref]
                    out_ref = refs[n]
                    at = pl.ds(aligned(begin(peer(a_ref[0], s, n_a)) + lo), size)
                    waits = [(), ()]
                    copies = []

                    def launch(source_ref, target_ref, sem):
                        copy = pltpu.make_async_copy(source_ref, target_ref, sem)
                        copy.start()
                        return copy

                    if initial and cold:
                        rows_ref, gain_ref, block_ref, sem = refs[n + 3 :]
                        first = [
                            launch(refs[3], rows_ref, sem.at[0]),
                            launch(refs[4], gain_ref, sem.at[1]),
                        ]
                        for k in range(2):
                            waits[k] = (
                                launch(weights[k].at[layer, at], block_ref.at[k], sem.at[2 + k]),
                            )
                        for copy in first:
                            copy.wait()
                        current = rows_ref[...].astype(F32)
                        lefts = [block_ref.at[0], block_ref.at[1]]
                    elif load:
                        stored, taps_ref = refs[n + 1 : n + 3], refs[n + 3]
                        raw_ref, turned_ref, sem = refs[n + 4 :]
                        raw = [
                            launch(refs[5 + k], raw_ref.at[k], sem.at[2 * n_a + k]) for k in range(2)
                        ]
                        blocks = [slice(None)]
                        if even:
                            targets = [s] + [t for t in range(n_a) if t != s]
                            blocks = [
                                pl.ds(aligned(begin(peer(a_ref[0], t, n_a))), piece)
                                for t in targets
                            ]
                        for i, block in enumerate(blocks):
                            for k in range(2):
                                copies.append(
                                    launch(
                                        weights[k].at[layer, block],
                                        stored[k].at[block],
                                        sem.at[2 * i + k],
                                    )
                                )
                        waits = [(copies[0],), (copies[1],)]
                        copies = copies[2:]
                        lefts = [ref.at[at] for ref in stored]
                    else:
                        lefts = [ref.at[at] for ref in weights]
                        if initial:
                            gain_ref, side_ref = refs[3 + n_p : 5 + n_p]
                            current = load_rows(refs[3 : 3 + n_p], side_ref, refs[n + 3])
                    if initial:
                        scaled_ref, tail_ref = refs[n + 1 : n + 3]
                        prepare(current, gain_ref[layer : layer + 1, :], scaled_ref, tail_ref)
                    else:
                        scaled_ref, tail_ref = refs[3:5]
                    scaled = scaled_ref[...]
                    for k in range(2):
                        for copy in waits[k]:
                            copy.wait()
                        out_ref[k * size : (k + 1) * size, :] = lax.dot_general(
                            lefts[k][...],
                            scaled,
                            (((1,), (1,)), ((), ())),
                            preferred_element_type=F32,
                        ).astype(BF16)
                    if h == 0:
                        out_ref[2 * size : 2 * size + EXTRA, :] = tail_ref[...]
                    if load:
                        for copy in raw:
                            copy.wait()
                        lines = [
                            raw_ref[kind, k, l : l + 1, :]
                            for l in range(layers)
                            for kind in range(2)
                            for k in range(kernel)
                        ]
                        if tap_rows > len(lines):
                            lines.append(jnp.zeros((tap_rows - len(lines), units), F32))
                        turned_ref[...] = jnp.concatenate(lines, axis=0).T
                        taps_ref[...] = turned_ref[pl.ds(aligned(begin(a_ref[0])), piece), :]
                    for copy in copies:
                        copy.wait()

                out = call(
                    body_fn,
                    args,
                    specs,
                    shapes,
                    4 * size * width * count,
                    4 * size * width,
                    scratch,
                )
                if initial:
                    extra = out[1:3]
                if load:
                    held, taps = out[1:3], out[3]
                outs[h, s] = out[0]
            return outs, taps

        def fetch(layer, sources, after):
            n = len(sources)

            def body_fn(*refs):
                sem = refs[-1]
                copies = []
                for k in range(n):
                    copy = pltpu.make_async_copy(refs[k].at[layer], refs[n + 1 + k], sem.at[k])
                    copy.start()
                    copies.append(copy)
                for copy in copies:
                    copy.wait()

            return call(
                body_fn,
                [*sources, after],
                [HBM] * n + [VMEM],
                [(source.shape[1:], BF16) for source in sources],
                2 * units * width * count // 3 * n,
                2 * n * units * width,
                [pltpu.SemaphoreType.DMA((n,))],
            )

        def act(layer, h, parts, inverse, taps):
            lo, size = cuts[h]
            first, last = h == 0, h == n_h - 1
            args = [*parts, taps] + ([] if first else [inverse])
            shapes = [((size, count), BF16)]
            if first and not last:
                shapes.append(((8, count), F32))

            def body_fn(*refs):
                parts_refs, taps_ref = refs[:n_a], refs[n_a]
                out_ref = refs[len(args)]
                total = parts_refs[0][...].astype(F32)
                for ref in parts_refs[1:]:
                    total = total + ref[...].astype(F32)
                if first:
                    tail = total[2 * size :]
                    scale = lax.rsqrt((tail[0:1] + tail[1:2]) / (width * n_a) + epsilon)
                    if not last:
                        refs[len(args) + 1][...] = jnp.broadcast_to(scale, (8, count))
                else:
                    scale = refs[n_a + 1][0:1, :]
                lin = total[: 2 * size] * scale
                lane = lax.broadcasted_iota(jnp.int32, (size, count), 1)

                def conv(kind):
                    result = None
                    for k in range(kernel):
                        shift = kernel - 1 - k
                        column = (layer * 2 + kind) * kernel + k
                        moved = lin[kind * size : (kind + 1) * size]
                        if shift:
                            moved = jnp.where(lane < shift, 0.0, pltpu.roll(moved, shift, 1))
                        term = taps_ref[lo : lo + size, column : column + 1] * moved
                        result = term if result is None else result + term
                    return result

                gate, value = conv(0), conv(1)
                out_ref[...] = (gate / (1.0 + jnp.exp(-gate)) * value).astype(BF16)

            out = call(
                body_fn,
                args,
                [VMEM] * len(args),
                shapes,
                60 * 2 * size * count,
                4 * n_a * size * count,
            )
            return out[0], (out[1] if len(out) > 1 else inverse)

        def term_of(left, weight, keep):
            if keep is not None:
                row = lax.broadcasted_iota(jnp.int32, left.shape, 0)
                left = jnp.where(row >= keep, left.astype(F32), 0.0).astype(BF16)
            return lax.dot_general(
                left, weight, (((0,), (0,)), ((), ())), preferred_element_type=F32
            )

        def down_own(weight, mine):
            def body_fn(weight_ref, a_ref, *refs):
                total = None
                p = a_ref[0]
                for h, (lo, size) in enumerate(cuts):
                    at = pl.ds(aligned(begin(p) + lo), size)
                    keep = None if even else p * piece - begin(p) - lo
                    term = term_of(refs[h][...], weight_ref[at, :], keep)
                    total = term if total is None else total + term
                refs[n_h][...] = total

            return call(
                body_fn,
                [weight, me_a, *mine],
                [VMEM, SMEM] + [VMEM] * n_h,
                [((count, width), F32)],
                2 * piece * width * count,
                2 * piece * width,
            )[0]

        def down(h, weight, total, others, picks, last):
            lo, size = cuts[h]
            n = len(picks)
            shapes = [((count, width), F32)]
            if last:
                shapes = [((half, width), BF16), ((half, width), F32)]

            def body_fn(weight_ref, sum_ref, a_ref, side_ref, *refs):
                total = sum_ref[...]
                for i, s in enumerate(picks):
                    p = source(a_ref[0], s, n_a)
                    at = pl.ds(aligned(begin(p) + lo), size)
                    keep = None if even else p * piece - begin(p) - lo
                    total = total + term_of(refs[i][...], weight_ref[at, :], keep)
                if not last:
                    refs[n][...] = total
                    return
                away_ref, kept_ref, hold_ref = refs[n:]
                hold_ref[...] = total
                side = side_ref[0] & 1
                away = hold_ref[pl.ds(aligned((1 - side) * half, half), half), :]
                away_ref[...] = away.astype(BF16)
                kept_ref[...] = hold_ref[pl.ds(aligned(side * half, half), half), :]

            return call(
                body_fn,
                [weight, total, me_a, me_c, *[others[s - 1] for s in picks]],
                [VMEM] * 2 + [SMEM] * 2 + [VMEM] * n,
                shapes,
                2 * size * n * width * count,
                2 * size * n * width,
                [pltpu.VMEM((count, width), F32)] if last else (),
            )

        def deal(kept, came):
            def body_fn(kept_ref, came_ref, z_ref, *refs):
                for s in range(n_z):
                    at = pl.ds(aligned(peer(z_ref[0] >> 1, s, n_z) * span), span)
                    value = kept_ref[at, :] + came_ref[at, :].astype(F32)
                    refs[s][...] = value.astype(refs[s].dtype)

            return call(
                body_fn,
                [kept, came, me_c],
                [VMEM, VMEM, SMEM],
                [((span, width), F32 if s == 0 else BF16) for s in range(n_z)],
                4 * half * width,
                8 * half * width,
            )

        def settle(layer, own, others, old):
            def body_fn(own_ref, *refs):
                at_ref, old_ref, out_ref = refs[-3:]
                branch = own_ref[...]
                for ref in refs[:-3]:
                    branch = branch + ref[...].astype(F32)
                if layer == 0:
                    at = (at_ref[0] & 1) * half + (at_ref[0] >> 1) * span
                    before = old_ref[pl.ds(aligned(at), span), :].astype(F32)
                else:
                    before = old_ref[...].astype(F32)
                out_ref[...] = (0.5 * before + branch).astype(BF16)

            return call(
                body_fn,
                [own, *others, me_c, old],
                [VMEM] * (1 + len(others)) + [SMEM, VMEM],
                [((span, width), BF16)],
                8 * span * width,
                8 * span * width,
            )[0]

        def gather(parts):
            def body_fn(*refs):
                z_ref, out_ref = refs[n_z:]
                for s in range(n_z):
                    at = pl.ds(aligned(source(z_ref[0] >> 1, s, n_z) * span), span)
                    out_ref[at, :] = refs[s][...]

            return call(
                body_fn,
                [*parts, me_c],
                [VMEM] * n_z + [SMEM],
                [((half, width), BF16)],
                half * width,
                4 * half * width,
            )[0]

        pieces = [tokens]
        old = tokens
        held = taps = None
        for layer in range(layers):
            outs, came_taps = up(layer, pieces, held)
            taps = taps if came_taps is None else came_taps
            (weight,) = fetch(layer, [down_rows], outs[n_h - 1, 0])
            inverse = None
            mine, others = [], []
            for h in range(n_h):
                parts = [outs[h, 0]]
                parts += [send_a(outs[h, s], s) for s in range(1, n_a)]
                hidden, inverse = act(layer, h, parts, inverse, taps)
                mine.append(hidden)
                others.append([send_a(hidden, s) for s in range(1, n_a)])
            total = down_own(weight, mine)
            turns = [(h, list(range(1, n_a))) for h in range(n_h)]
            if n_a == 4:
                turns = turns[:-1] + [(n_h - 1, [3, 1]), (n_h - 1, [2])]
            for i, (h, picks) in enumerate(turns):
                out = down(h, weight, total, others[h], picks, i == len(turns) - 1)
                total = out[0]
            away, kept = out
            dealt = deal(kept, send_core(away))
            came = [send_z(dealt[s], s) for s in range(1, n_z)]
            if layer + 1 < layers:
                ahead = [gate_rows, value_rows]
                held = fetch(layer + 1, ahead, dealt[0])
            old = settle(layer, dealt[0], came, old)
            near = gather([old] + [send_z(old, s) for s in range(1, n_z)])
            pieces = [near, send_core(near)]

        def place(rows, flip, made):
            def body_fn(*refs):
                rows_ref, side_ref, out_ref, sem = refs[0], refs[1], refs[-2], refs[-1]
                side = (side_ref[0] & 1) ^ flip
                at = pl.ds(aligned(side * half, half), half)
                copy = pltpu.make_async_copy(rows_ref, out_ref.at[at], sem)
                copy.start()
                copy.wait()

            args, specs, alias = [rows, me_c], [VMEM, SMEM], {}
            if made is not None:
                args, specs, alias = args + [made], specs + [HBM], {2: 0}
            return pl.pallas_call(
                body_fn,
                in_specs=specs,
                out_specs=HBM,
                out_shape=jax.ShapeDtypeStruct((count, width), BF16),
                scratch_shapes=[pltpu.SemaphoreType.DMA],
                input_output_aliases=alias,
                cost_estimate=pl.CostEstimate(
                    flops=half * width, bytes_accessed=4 * half * width, transcendentals=0
                ),
                compiler_params=pltpu.CompilerParams(vmem_limit_bytes=16 * MIB),
            )(*args)

        near, far = pieces
        return place(far, 1, place(near, 0, None))

    return body


def solution(mesh):
    return jax.shard_map(
        make_body(mesh),
        mesh=mesh,
        in_specs=(
            P(None, "ra"),
            P(None, "ra"),
            P(None, "ra", "cb"),
            P(None, "ra", "cb"),
            P(None, None, "cb"),
            P(None, None, "cb"),
            P(None, "cb", "ra"),
        ),
        out_specs=P(None, "ra"),
        check_vma=False,
    )
```

```python
import jax
import jax.numpy as jnp
from jax import lax
from jax.experimental import pallas as pl
from jax.experimental.pallas import tpu as pltpu
from jax.sharding import PartitionSpec as P


epsilon = 1e-06
F32 = jnp.float32
BF16 = jnp.bfloat16
EXTRA = 8
SPLITS = 2
MIB = 1 << 20
VMEM = pl.BlockSpec(memory_space=pltpu.VMEM)
SMEM = pl.BlockSpec(memory_space=pltpu.SMEM)
HBM = pl.BlockSpec(memory_space=pltpu.HBM)


def piece_of(units, members):
    return -(-(-(-units // members)) // 8) * 8


def splits_of(piece):
    return SPLITS if piece >= 128 else 1


def call(body, args, specs, shapes, flops, moved, scratch=(), room=16):
    return pl.pallas_call(
        body,
        in_specs=specs,
        out_specs=[VMEM] * len(shapes),
        out_shape=[jax.ShapeDtypeStruct(*shape) for shape in shapes],
        scratch_shapes=scratch,
        cost_estimate=pl.CostEstimate(
            flops=int(flops), bytes_accessed=int(moved), transcendentals=0
        ),
        compiler_params=pltpu.CompilerParams(vmem_limit_bytes=room * MIB),
    )(*args)


def aligned(value, step=8):
    return pl.multiple_of(value, step)


def prepare(current, gain, scaled_ref, tail_ref):
    scaled_ref[...] = (current * gain).astype(BF16)
    squares = current * current
    folded = squares[:, :128]
    for k in range(1, squares.shape[1] // 128):
        folded = folded + squares[:, k * 128 : (k + 1) * 128]
    total = jnp.sum(folded.T, axis=0, keepdims=True)
    high = total.astype(BF16).astype(F32)
    low = total - high
    row = lax.broadcasted_iota(jnp.int32, (EXTRA, total.shape[1]), 0)
    tail_ref[...] = jnp.where(row == 0, high, jnp.where(row == 1, low, 0.0)).astype(BF16)


def load_rows(pieces, side_ref, rows_ref):
    if len(pieces) == 1:
        return pieces[0][...].astype(F32)
    near, far = pieces
    half = near.shape[0]
    side = side_ref[0] & 1
    rows_ref[pl.ds(aligned(side * half, half), half), :] = near[...]
    rows_ref[pl.ds(aligned((1 - side) * half, half), half), :] = far[...]
    return rows_ref[...].astype(F32)


def make_body(mesh):
    n_a = mesh.shape["ra"]
    n_c = mesh.shape["cb"]
    n_z = n_c // 2

    def peer(i, s, n):
        return i ^ s if n & (n - 1) == 0 else (i + s) % n

    def source(i, s, n):
        return i ^ s if n & (n - 1) == 0 else (i - s) % n

    def send_a(value, s):
        return lax.ppermute(value, "ra", [(i, peer(i, s, n_a)) for i in range(n_a)])

    def send_z(value, s):
        pairs = [(z * 2 + k, peer(z, s, n_z) * 2 + k) for z in range(n_z) for k in range(2)]
        return lax.ppermute(value, "cb", pairs)

    def send_core(value):
        return lax.ppermute(value, "cb", [(i, i ^ 1) for i in range(n_c)])

    def body(tokens, norm_gain, gate_weight, value_weight, gate_taps, value_taps, down_weight):
        layers, width, units = gate_weight.shape
        kernel = gate_taps.shape[1]
        count = tokens.shape[0]
        piece = piece_of(units, n_a)
        splits = splits_of(piece)
        step = piece if splits == 1 else -(-2 * piece // 24) * 8
        cuts = [(lo, min(step, piece - lo)) for lo in range(0, piece, step)]
        n_h = len(cuts)
        even = n_a * piece == units
        a = lax.axis_index("ra")
        c = lax.axis_index("cb")
        half = count // 2
        span = half // n_z

        def begin(p):
            return jnp.minimum(p * piece, units - piece)

        def scalar(value):
            return value.astype(jnp.int32).reshape(1)

        me_a, me_c = scalar(a), scalar(c)

        def stay(value):
            return pltpu.with_memory_space_constraint(value, pltpu.HBM)

        gate_rows = stay(gate_weight.transpose(0, 2, 1))
        value_rows = stay(value_weight.transpose(0, 2, 1))
        down_rows = stay(down_weight)

        tap_rows = 2 * kernel * layers
        tap_rows += -tap_rows % 8
        tap_args = [gate_taps.transpose(1, 0, 2), value_taps.transpose(1, 0, 2)]

        sends = list(range(n_a - 1, 0, -1))
        order = [(h, s) for h in range(n_h) for s in sends] + [(h, 0) for h in range(n_h)]

        def up(layer, pieces, held):
            outs = {}
            extra = taps = None
            n_p = len(pieces)
            cold = held is None
            for index, (h, s) in enumerate(order):
                lo, size = cuts[h]
                rows = 2 * size + (EXTRA if h == 0 else 0)
                initial = index == 0
                load = cold and index == 1
                args = [me_a, *(held or (gate_rows, value_rows))]
                specs = [SMEM] + [VMEM if held else HBM] * 2
                shapes = [((rows, count), BF16)]
                scratch = []
                if initial and cold:
                    args += [stay(pieces[0]), stay(norm_gain), me_c]
                    specs += [HBM, HBM, SMEM]
                elif initial:
                    args += [*pieces, norm_gain, me_c]
                    specs += [VMEM] * (n_p + 1) + [SMEM]
                else:
                    args += extra
                    specs += [VMEM] * 2
                if initial:
                    shapes += [((count, width), BF16), ((EXTRA, count), BF16)]
                    scratch.append(pltpu.VMEM((count, width), BF16))
                if initial and cold:
                    scratch += [
                        pltpu.VMEM(norm_gain.shape, F32),
                        pltpu.VMEM((2, size, width), BF16),
                        pltpu.SemaphoreType.DMA((4,)),
                    ]
                if load:
                    args += [stay(value) for value in tap_args]
                    specs += [HBM, HBM]
                    shapes += [((units, width), BF16)] * 2 + [((piece, tap_rows), F32)]
                    scratch += [
                        pltpu.VMEM((2, *tap_args[0].shape), F32),
                        pltpu.VMEM((units, tap_rows), F32),
                        pltpu.SemaphoreType.DMA((2 * n_a + 2,)),
                    ]

                def body_fn(
                    *refs, s=s, lo=lo, size=size, h=h, initial=initial, load=load, n=len(args)
                ):
                    a_ref, gate_ref, value_ref = refs[:3]
                    weights = [gate_ref, value_ref]
                    out_ref = refs[n]
                    at = pl.ds(aligned(begin(peer(a_ref[0], s, n_a)) + lo), size)
                    waits = [(), ()]
                    copies = []

                    def launch(source_ref, target_ref, sem):
                        copy = pltpu.make_async_copy(source_ref, target_ref, sem)
                        copy.start()
                        return copy

                    if initial and cold:
                        rows_ref, gain_ref, block_ref, sem = refs[n + 3 :]
                        first = [
                            launch(refs[3], rows_ref, sem.at[0]),
                            launch(refs[4], gain_ref, sem.at[1]),
                        ]
                        for k in range(2):
                            waits[k] = (
                                launch(weights[k].at[layer, at], block_ref.at[k], sem.at[2 + k]),
                            )
                        for copy in first:
                            copy.wait()
                        current = rows_ref[...].astype(F32)
                        lefts = [block_ref.at[0], block_ref.at[1]]
                    elif load:
                        stored, taps_ref = refs[n + 1 : n + 3], refs[n + 3]
                        raw_ref, turned_ref, sem = refs[n + 4 :]
                        raw = [
                            launch(refs[5 + k], raw_ref.at[k], sem.at[2 * n_a + k]) for k in range(2)
                        ]
                        blocks = [slice(None)]
                        if even:
                            targets = [s] + [t for t in range(n_a) if t != s]
                            blocks = [
                                pl.ds(aligned(begin(peer(a_ref[0], t, n_a))), piece)
                                for t in targets
                            ]
                        for i, block in enumerate(blocks):
                            for k in range(2):
                                copies.append(
                                    launch(
                                        weights[k].at[layer, block],
                                        stored[k].at[block],
                                        sem.at[2 * i + k],
                                    )
                                )
                        waits = [(copies[0],), (copies[1],)]
                        copies = copies[2:]
                        lefts = [ref.at[at] for ref in stored]
                    else:
                        lefts = [ref.at[at] for ref in weights]
                        if initial:
                            gain_ref, side_ref = refs[3 + n_p : 5 + n_p]
                            current = load_rows(refs[3 : 3 + n_p], side_ref, refs[n + 3])
                    if initial:
                        scaled_ref, tail_ref = refs[n + 1 : n + 3]
                        prepare(current, gain_ref[layer : layer + 1, :], scaled_ref, tail_ref)
                    else:
                        scaled_ref, tail_ref = refs[3:5]
                    scaled = scaled_ref[...]
                    for k in range(2):
                        for copy in waits[k]:
                            copy.wait()
                        out_ref[k * size : (k + 1) * size, :] = lax.dot_general(
                            lefts[k][...],
                            scaled,
                            (((1,), (1,)), ((), ())),
                            preferred_element_type=F32,
                        ).astype(BF16)
                    if h == 0:
                        out_ref[2 * size : 2 * size + EXTRA, :] = tail_ref[...]
                    if load:
                        for copy in raw:
                            copy.wait()
                        lines = [
                            raw_ref[kind, k, l : l + 1, :]
                            for l in range(layers)
                            for kind in range(2)
                            for k in range(kernel)
                        ]
                        if tap_rows > len(lines):
                            lines.append(jnp.zeros((tap_rows - len(lines), units), F32))
                        turned_ref[...] = jnp.concatenate(lines, axis=0).T
                        taps_ref[...] = turned_ref[pl.ds(aligned(begin(a_ref[0])), piece), :]
                    for copy in copies:
                        copy.wait()

                out = call(
                    body_fn,
                    args,
                    specs,
                    shapes,
                    4 * size * width * count,
                    4 * size * width,
                    scratch,
                )
                if initial:
                    extra = out[1:3]
                if load:
                    held, taps = out[1:3], out[3]
                outs[h, s] = out[0]
            return outs, taps

        def fetch(layer, sources, after):
            n = len(sources)

            def body_fn(*refs):
                sem = refs[-1]
                copies = []
                for k in range(n):
                    copy = pltpu.make_async_copy(refs[k].at[layer], refs[n + 1 + k], sem.at[k])
                    copy.start()
                    copies.append(copy)
                for copy in copies:
                    copy.wait()

            return call(
                body_fn,
                [*sources, after],
                [HBM] * n + [VMEM],
                [(source.shape[1:], BF16) for source in sources],
                2 * units * width * count // 3 * n,
                2 * n * units * width,
                [pltpu.SemaphoreType.DMA((n,))],
            )

        def act(layer, h, parts, inverse, taps):
            lo, size = cuts[h]
            first, last = h == 0, h == n_h - 1
            args = [*parts, taps] + ([] if first else [inverse])
            shapes = [((size, count), BF16)]
            if first and not last:
                shapes.append(((8, count), F32))

            def body_fn(*refs):
                parts_refs, taps_ref = refs[:n_a], refs[n_a]
                out_ref = refs[len(args)]
                total = parts_refs[0][...].astype(F32)
                for ref in parts_refs[1:]:
                    total = total + ref[...].astype(F32)
                if first:
                    tail = total[2 * size :]
                    scale = lax.rsqrt((tail[0:1] + tail[1:2]) / (width * n_a) + epsilon)
                    if not last:
                        refs[len(args) + 1][...] = jnp.broadcast_to(scale, (8, count))
                else:
                    scale = refs[n_a + 1][0:1, :]
                lin = total[: 2 * size] * scale
                lane = lax.broadcasted_iota(jnp.int32, (size, count), 1)

                def conv(kind):
                    result = None
                    for k in range(kernel):
                        shift = kernel - 1 - k
                        column = (layer * 2 + kind) * kernel + k
                        moved = lin[kind * size : (kind + 1) * size]
                        if shift:
                            moved = jnp.where(lane < shift, 0.0, pltpu.roll(moved, shift, 1))
                        term = taps_ref[lo : lo + size, column : column + 1] * moved
                        result = term if result is None else result + term
                    return result

                gate, value = conv(0), conv(1)
                out_ref[...] = (gate / (1.0 + jnp.exp(-gate)) * value).astype(BF16)

            out = call(
                body_fn,
                args,
                [VMEM] * len(args),
                shapes,
                60 * 2 * size * count,
                4 * n_a * size * count,
            )
            return out[0], (out[1] if len(out) > 1 else inverse)

        def term_of(left, weight, keep):
            if keep is not None:
                row = lax.broadcasted_iota(jnp.int32, left.shape, 0)
                left = jnp.where(row >= keep, left.astype(F32), 0.0).astype(BF16)
            return lax.dot_general(
                left, weight, (((0,), (0,)), ((), ())), preferred_element_type=F32
            )

        def down_own(weight, mine):
            def body_fn(weight_ref, a_ref, *refs):
                total = None
                p = a_ref[0]
                for h, (lo, size) in enumerate(cuts):
                    at = pl.ds(aligned(begin(p) + lo), size)
                    keep = None if even else p * piece - begin(p) - lo
                    term = term_of(refs[h][...], weight_ref[at, :], keep)
                    total = term if total is None else total + term
                refs[n_h][...] = total

            return call(
                body_fn,
                [weight, me_a, *mine],
                [VMEM, SMEM] + [VMEM] * n_h,
                [((count, width), F32)],
                2 * piece * width * count,
                2 * piece * width,
            )[0]

        def down(h, weight, total, others, picks, last):
            lo, size = cuts[h]
            n = len(picks)
            shapes = [((count, width), F32)]
            if last:
                shapes = [((half, width), BF16), ((half, width), F32)]

            def body_fn(weight_ref, sum_ref, a_ref, side_ref, *refs):
                total = sum_ref[...]
                for i, s in enumerate(picks):
                    p = source(a_ref[0], s, n_a)
                    at = pl.ds(aligned(begin(p) + lo), size)
                    keep = None if even else p * piece - begin(p) - lo
                    total = total + term_of(refs[i][...], weight_ref[at, :], keep)
                if not last:
                    refs[n][...] = total
                    return
                away_ref, kept_ref, hold_ref = refs[n:]
                hold_ref[...] = total
                side = side_ref[0] & 1
                away = hold_ref[pl.ds(aligned((1 - side) * half, half), half), :]
                away_ref[...] = away.astype(BF16)
                kept_ref[...] = hold_ref[pl.ds(aligned(side * half, half), half), :]

            return call(
                body_fn,
                [weight, total, me_a, me_c, *[others[s - 1] for s in picks]],
                [VMEM] * 2 + [SMEM] * 2 + [VMEM] * n,
                shapes,
                2 * size * n * width * count,
                2 * size * n * width,
                [pltpu.VMEM((count, width), F32)] if last else (),
            )

        def down_half(h, weight, total, others, s, flip):
            lo, size = cuts[h]

            def body_fn(weight_ref, sum_ref, a_ref, side_ref, hidden_ref, out_ref):
                side = (side_ref[0] & 1) ^ flip
                mine = pl.ds(aligned(side * half, half), half)
                p = source(a_ref[0], s, n_a)
                at = pl.ds(aligned(begin(p) + lo), size)
                keep = None if even else p * piece - begin(p) - lo
                term = term_of(hidden_ref[:, mine], weight_ref[at, :], keep)
                out_ref[...] = (sum_ref[mine, :] + term).astype(out_ref.dtype)

            return call(
                body_fn,
                [weight, total, me_a, me_c, others[s - 1]],
                [VMEM] * 2 + [SMEM] * 2 + [VMEM],
                [((half, width), BF16 if flip else F32)],
                2 * size * half * width,
                2 * size * width,
            )[0]

        def deal(kept, came):
            def body_fn(kept_ref, came_ref, z_ref, *refs):
                for s in range(n_z):
                    at = pl.ds(aligned(peer(z_ref[0] >> 1, s, n_z) * span), span)
                    value = kept_ref[at, :] + came_ref[at, :].astype(F32)
                    refs[s][...] = value.astype(refs[s].dtype)

            return call(
                body_fn,
                [kept, came, me_c],
                [VMEM, VMEM, SMEM],
                [((span, width), F32 if s == 0 else BF16) for s in range(n_z)],
                4 * half * width,
                8 * half * width,
            )

        def settle(layer, own, others, old):
            def body_fn(own_ref, *refs):
                at_ref, old_ref, out_ref = refs[-3:]
                branch = own_ref[...]
                for ref in refs[:-3]:
                    branch = branch + ref[...].astype(F32)
                if layer == 0:
                    at = (at_ref[0] & 1) * half + (at_ref[0] >> 1) * span
                    before = old_ref[pl.ds(aligned(at), span), :].astype(F32)
                else:
                    before = old_ref[...].astype(F32)
                out_ref[...] = (0.5 * before + branch).astype(BF16)

            return call(
                body_fn,
                [own, *others, me_c, old],
                [VMEM] * (1 + len(others)) + [SMEM, VMEM],
                [((span, width), BF16)],
                8 * span * width,
                8 * span * width,
            )[0]

        def gather(parts):
            def body_fn(*refs):
                z_ref, out_ref = refs[n_z:]
                for s in range(n_z):
                    at = pl.ds(aligned(source(z_ref[0] >> 1, s, n_z) * span), span)
                    out_ref[at, :] = refs[s][...]

            return call(
                body_fn,
                [*parts, me_c],
                [VMEM] * n_z + [SMEM],
                [((half, width), BF16)],
                half * width,
                4 * half * width,
            )[0]

        pieces = [tokens]
        old = tokens
        held = taps = None
        for layer in range(layers):
            outs, came_taps = up(layer, pieces, held)
            taps = taps if came_taps is None else came_taps
            (weight,) = fetch(layer, [down_rows], outs[n_h - 1, 0])
            inverse = None
            mine, others = [], []
            for h in range(n_h):
                parts = [outs[h, 0]]
                parts += [send_a(outs[h, s], s) for s in range(1, n_a)]
                hidden, inverse = act(layer, h, parts, inverse, taps)
                mine.append(hidden)
                others.append([send_a(hidden, s) for s in range(1, n_a)])
            total = down_own(weight, mine)
            turns = [(h, list(range(1, n_a))) for h in range(n_h)]
            if n_a == 4:
                turns = turns[:-1] + [(n_h - 1, [3, 1]), (n_h - 1, [2])]
            halves = n_a == 4 and half % 128 == 0
            for i, (h, picks) in enumerate(turns[: len(turns) - halves]):
                out = down(h, weight, total, others[h], picks, i == len(turns) - 1)
                total = out[0]
            if halves:
                h, (s,) = turns[-1]
                out = [down_half(h, weight, total, others[h], s, flip) for flip in (1, 0)]
            away, kept = out
            dealt = deal(kept, send_core(away))
            came = [send_z(dealt[s], s) for s in range(1, n_z)]
            if layer + 1 < layers:
                ahead = [gate_rows, value_rows]
                held = fetch(layer + 1, ahead, dealt[0])
            old = settle(layer, dealt[0], came, old)
            near = gather([old] + [send_z(old, s) for s in range(1, n_z)])
            pieces = [near, send_core(near)]

        def place(rows, flip, made):
            def body_fn(*refs):
                rows_ref, side_ref, out_ref, sem = refs[0], refs[1], refs[-2], refs[-1]
                side = (side_ref[0] & 1) ^ flip
                at = pl.ds(aligned(side * half, half), half)
                copy = pltpu.make_async_copy(rows_ref, out_ref.at[at], sem)
                copy.start()
                copy.wait()

            args, specs, alias = [rows, me_c], [VMEM, SMEM], {}
            if made is not None:
                args, specs, alias = args + [made], specs + [HBM], {2: 0}
            return pl.pallas_call(
                body_fn,
                in_specs=specs,
                out_specs=HBM,
                out_shape=jax.ShapeDtypeStruct((count, width), BF16),
                scratch_shapes=[pltpu.SemaphoreType.DMA],
                input_output_aliases=alias,
                cost_estimate=pl.CostEstimate(
                    flops=half * width, bytes_accessed=4 * half * width, transcendentals=0
                ),
                compiler_params=pltpu.CompilerParams(vmem_limit_bytes=16 * MIB),
            )(*args)

        near, far = pieces
        return place(far, 1, place(near, 0, None))

    return body


def solution(mesh):
    return jax.shard_map(
        make_body(mesh),
        mesh=mesh,
        in_specs=(
            P(None, "ra"),
            P(None, "ra"),
            P(None, "ra", "cb"),
            P(None, "ra", "cb"),
            P(None, None, "cb"),
            P(None, None, "cb"),
            P(None, "cb", "ra"),
        ),
        out_specs=P(None, "ra"),
        check_vma=False,
    )
```
